256 devices in a mesh: rep: 2 (over z_hi), fs: 16 (over z_lo, x), tp: 8 (over y, core).
Axes of the slice: x: 4, y: 4, z: 8 (z_hi: 2, z_lo: 4; z = z_hi * 4 + z_lo), core: 2. Of those that a mesh axis runs over, the one named last changes fastest.
Arguments:
- tokens: bfloat16 [32768, 2048], P(('rep', 'fs', 'tp')), may hold values from -6 to 6
- mix_gain: float32 [2048], replicated, may hold values from 0.1 to 1.9
- w_query: bfloat16 [2048, 1024], P('fs', 'tp'), may hold values from -0.125 to 0.125
- w_key: bfloat16 [2048, 1024], P('fs', 'tp'), may hold values from -0.125 to 0.125
- w_value: bfloat16 [2048, 2048], P('fs', 'tp'), may hold values from -0.125 to 0.125
- w_decay_down: bfloat16 [2048, 32], replicated, may hold values from -0.125 to 0.125
- w_decay_up: bfloat16 [32, 1024], replicated, may hold values from -2 to 2
- decay_bias: float32 [1024], replicated, may hold values from -1 to 6
- decay_shift: float32 [32768, 1024], P(('rep', 'fs'), 'tp'), may hold values from -3 to 0
- head_gain: float32 [2048], replicated, may hold values from 0.1 to 1.9
- w_mix_out: bfloat16 [2048, 2048], P('tp', 'fs'), may hold values from -0.125 to 0.125
- ffn_gain: float32 [2048], replicated, may hold values from 0.1 to 1.9
- w_gate: bfloat16 [2048, 5632], P('fs', 'tp'), may hold values from -0.125 to 0.125
- w_up: bfloat16 [2048, 5632], P('fs', 'tp'), may hold values from -0.125 to 0.125
- w_down: bfloat16 [5632, 2048], P('tp', 'fs'), may hold values from -0.078125 to 0.078125
Outputs:
- layer_out: float32 [32768, 2048], P(('rep', 'fs', 'tp'))
The draws below stay inside these ranges and needn't reach their ends.
All inputs are finite; a program needn't handle non-finite values.
Results may differ from the reference program's by a relative error of at most 0.04.
Values may be sent and summed in bfloat16 or wider, within the bound.
A program may use at most 128 MiB of HBM per device.

```python
import jax
import jax.numpy as jnp
from jax import lax

D = 2048
HEADS = 8
KEY_CHANNELS = 128
DV = 256
KEY = 1024
RANK = 32
FF = 5632
BLK = 64
SEQUENCE_LENGTH = 1024
TOKENS = 32768
N_TP = 8


def draw_decay_bias(key, part):
    head_key, fast_key, slow_key = jax.random.split(key, 3)
    fast_chance = 0.5
    fast_heads = jax.random.bernoulli(head_key, fast_chance, (HEADS,))
    fast_values = jax.random.uniform(fast_key, (HEADS, KEY_CHANNELS), jnp.float32, -0.5, 1.5)
    slow_values = jax.random.uniform(slow_key, (HEADS, KEY_CHANNELS), jnp.float32, 4.0, 6.0)
    return jnp.where(fast_heads[:, None], fast_values, slow_values).reshape(KEY).astype(jnp.float32)


def draw_decay_shift(key, part):
    sequence_count = TOKENS // SEQUENCE_LENGTH
    location_key, depth_key, rate_key = jax.random.split(key, 3)
    spike_locations = jax.random.randint(location_key, (sequence_count, 3), 0, SEQUENCE_LENGTH)
    spike_magnitudes = jnp.log(jax.random.uniform(depth_key, (sequence_count, 3, HEADS), jnp.float32, 0.5, 0.8))
    row_ids = jnp.arange(TOKENS)
    sequence_index = row_ids // SEQUENCE_LENGTH
    token_positions = row_ids % SEQUENCE_LENGTH
    match_flags = (token_positions[:, None] == spike_locations[sequence_index]).astype(jnp.float32)
    spike_events = jnp.einsum('fi,fit->ft', match_flags, spike_magnitudes[sequence_index])
    block_count = TOKENS // BLK
    rates = -jnp.exp(jax.random.uniform(rate_key, (block_count, KEY), jnp.float32, jnp.log(0.3), jnp.log(3.0))) / SEQUENCE_LENGTH
    decay_rate_rows = jnp.repeat(rates, BLK, axis=0)
    return (jnp.repeat(spike_events, KEY_CHANNELS, axis=1) + decay_rate_rows).astype(jnp.float32)


def shard_levels(stream_key, dims, cuts, smallest, top_value):
    level, own = 1.0, jax.random.fold_in(stream_key, 6)
    for position, parts in cuts:
        heights = jnp.exp(jax.random.uniform(jax.random.fold_in(own, position), (parts,), jnp.float32, smallest / len(cuts), top_value / len(cuts)))
        level = level * jnp.repeat(heights, dims[position] // parts).reshape([-1 if axis == position else 1 for axis in range(len(dims))])
    return level


def scatter_about(stream_key, shape, spread, bound, cuts=(), dtype=jnp.bfloat16):
    drawn = spread * jax.random.normal(stream_key, shape, jnp.float32)
    if cuts:
        drawn = drawn * shard_levels(stream_key, shape, cuts, -0.22, 0.18)
    return jnp.clip(drawn, -bound, bound).astype(dtype)


def setup_inputs(seed: int = 0) -> dict:
    streams_of = jax.random.split(jax.random.key(seed), 16)
    return {
        "tokens": scatter_about(streams_of[0], (TOKENS, D), 1.0, 6.0, ((0, 256),)),
        "mix_gain": jnp.clip(1.0 + 0.18 * jax.random.normal(streams_of[1], (D,), jnp.float32), 0.1, 1.9),
        "w_query": scatter_about(streams_of[2], (D, KEY), D ** -0.5, 0.125, ((0, 16), (1, 8))),
        "w_key": scatter_about(streams_of[3], (D, KEY), D ** -0.5, 0.125, ((0, 16), (1, 8))),
        "w_value": scatter_about(streams_of[4], (D, D), D ** -0.5, 0.125, ((0, 16), (1, 8))),
        "w_decay_down": scatter_about(streams_of[5], (D, RANK), D ** -0.5, 0.125),
        "w_decay_up": scatter_about(streams_of[6], (RANK, KEY), (RANK // 4) ** -0.5, 2.0),
        "decay_bias": draw_decay_bias(jax.random.fold_in(streams_of[15], 71), 0),
        "decay_shift": draw_decay_shift(jax.random.fold_in(streams_of[15], 71), 0),
        "head_gain": jnp.clip(1.0 + 0.18 * jax.random.normal(streams_of[9], (D,), jnp.float32), 0.1, 1.9),
        "w_mix_out": scatter_about(streams_of[10], (D, D), D ** -0.5, 0.125, ((0, 8), (1, 16))),
        "ffn_gain": jnp.clip(1.0 + 0.18 * jax.random.normal(streams_of[11], (D,), jnp.float32), 0.1, 1.9),
        "w_gate": scatter_about(streams_of[12], (D, FF), D ** -0.5, 0.125, ((0, 16), (1, 8))),
        "w_up": scatter_about(streams_of[13], (D, FF), D ** -0.5, 0.125, ((0, 16), (1, 8))),
        "w_down": scatter_about(streams_of[14], (FF, D), FF ** -0.5, 0.078125, ((0, 8), (1, 16))),
    }


EPS = 1e-06
TAU = 16.0

def rms_norm(values, gain):
    return values * lax.rsqrt(lax.optimization_barrier(jnp.mean(values * values, axis=-1, keepdims=True)) + EPS) * gain

def recurrence(query_proj, key_proj, value_proj, log_decay):
    blocks = SEQUENCE_LENGTH // BLK
    queries = query_proj.astype(jnp.float32).reshape(blocks, BLK, HEADS, KEY_CHANNELS) * KEY_CHANNELS ** (-0.5)
    keys = key_proj.astype(jnp.float32).reshape(blocks, BLK, HEADS, KEY_CHANNELS)
    values = value_proj.astype(jnp.float32).reshape(blocks, BLK, HEADS, DV)
    decays = log_decay.reshape(blocks, BLK, HEADS, KEY_CHANNELS)
    cumul = jnp.cumsum(decays, axis=1)
    totals = cumul[:, -1]
    weighted = keys * jnp.exp(totals[:, None] - cumul)
    updates = jnp.einsum('bchd,bche->bhde', weighted, values, precision=lax.Precision.HIGHEST)

    def advance(state, inputs):
        total, update = inputs
        new_state = jnp.exp(total)[..., None] * state + update
        return (new_state, state)
    _, previous = lax.scan(advance, jnp.zeros((HEADS, KEY_CHANNELS, DV), jnp.float32), (totals, updates))
    q_decayed = queries * jnp.exp(cumul)
    k_decayed = keys * jnp.exp(-cumul)
    scores = jnp.einsum('bchd,bshd->bhcs', q_decayed, k_decayed, precision=lax.Precision.HIGHEST)
    causal = (jnp.arange(BLK)[:, None] >= jnp.arange(BLK)[None, :]).astype(jnp.float32)
    scores = scores * causal
    inner = jnp.einsum('bhcs,bshe->bche', scores, values, precision=lax.Precision.HIGHEST)
    carried = jnp.einsum('bchd,bhde->bche', q_decayed, previous, precision=lax.Precision.HIGHEST)
    return (inner + carried).reshape(SEQUENCE_LENGTH, HEADS, DV)

def reference(tokens, mix_gain, w_query, w_key, w_value, w_decay_down, w_decay_up, decay_bias, decay_shift, head_gain, w_mix_out, ffn_gain, w_gate, w_up, w_down):
    sequence_count = TOKENS // SEQUENCE_LENGTH
    out_groups = w_mix_out.astype(jnp.float32).reshape(N_TP, D // N_TP, D)
    down_groups = w_down.astype(jnp.float32).reshape(N_TP, FF // N_TP, D)

    def layer(inputs):
        seq_tokens, seq_shift = inputs
        source = seq_tokens.astype(jnp.float32)
        normed = rms_norm(source, mix_gain).astype(jnp.bfloat16)
        query_proj = jnp.dot(normed, w_query, preferred_element_type=jnp.float32).astype(jnp.bfloat16)
        key_proj = jnp.dot(normed, w_key, preferred_element_type=jnp.float32).astype(jnp.bfloat16)
        value_proj = jnp.dot(normed, w_value, preferred_element_type=jnp.float32).astype(jnp.bfloat16)
        low_rank = jnp.dot(normed, w_decay_down, preferred_element_type=jnp.float32).astype(jnp.bfloat16)
        pre_decay = jnp.dot(low_rank, w_decay_up, preferred_element_type=jnp.float32) + decay_bias
        log_decay = jax.nn.log_sigmoid(pre_decay) / TAU + seq_shift
        head_out = recurrence(query_proj, key_proj, value_proj, log_decay)
        gated = rms_norm(head_out, head_gain.reshape(HEADS, DV)).astype(jnp.bfloat16)
        gated = gated.reshape(SEQUENCE_LENGTH, N_TP, D // N_TP).astype(jnp.float32)
        partials = jnp.einsum('lgc,gcd->gld', gated, out_groups).astype(jnp.bfloat16)
        hidden = source + lax.optimization_barrier(jnp.sum(partials.astype(jnp.float32), axis=0))
        normed_ffn = rms_norm(hidden, ffn_gain).astype(jnp.bfloat16)
        gate_proj = jnp.dot(normed_ffn, w_gate, preferred_element_type=jnp.float32)
        up_proj = jnp.dot(normed_ffn, w_up, preferred_element_type=jnp.float32)
        activated = (jax.nn.silu(gate_proj) * up_proj).astype(jnp.bfloat16)
        activated = activated.reshape(SEQUENCE_LENGTH, N_TP, FF // N_TP).astype(jnp.float32)
        ffn_parts = jnp.einsum('lgc,gcd->gld', activated, down_groups).astype(jnp.bfloat16)
        return hidden + lax.optimization_barrier(jnp.sum(ffn_parts.astype(jnp.float32), axis=0))
    result = lax.map(layer, (tokens.reshape(sequence_count, SEQUENCE_LENGTH, D), decay_shift.reshape(sequence_count, SEQUENCE_LENGTH, KEY)))
    return result.reshape(TOKENS, D)
```

```python
import jax
import jax.numpy as jnp
from jax import lax
from jax.experimental import pallas as pl
from jax.experimental.pallas import tpu as pltpu
from jax.sharding import Mesh
from jax.sharding import PartitionSpec as P

AXES = ("rep", "fz", "fx", "ty", "tc")
MESH = pl.DeviceIdType.MESH
KEY_CHANNELS = 128
DV = 256
BLK = 64
EPS = 1e-06
TAU = 16.0
F32 = jnp.float32
BF16 = jnp.bfloat16
QKV, OUT, GATE, UP, DOWN = range(5)


def rms_norm(values, gain):
    return values * lax.rsqrt(jnp.mean(values * values, axis=-1, keepdims=True) + EPS) * gain


def dot(a, b, dims=(((1,), (0,)), ((), ()))):
    return lax.dot_general(a, b, dims, preferred_element_type=F32)


def order(i):
    return jnp.where(i < 2, i, 5 - i)


def kernel(
    tokens_hbm, shift_hbm, wq_hbm, wk_hbm, wv_hbm, wo_hbm, wg_hbm, wu_hbm, wd_hbm,
    mix_gain, ffn_gain, head_gain, down_proj, up_proj, bias,
    out,
    wqkv, wo, wg, wu, wd,
    tok, shift, n1, n2, qs, ks, vs, gated, state, hidden, act,
    keep1, send1, cross1, recv1, keep2, send2, cross2, recv2,
    loc_sem, w_send, w_recv,
    ag1_send, ag1_recv, ag2_send, ag2_recv,
    x1_send, x1_recv, r1_send, r1_recv, x2_send, x2_recv, r2_send, r2_recv,
):
    rep, fz, fx = lax.axis_index("rep"), lax.axis_index("fz"), lax.axis_index("fx")
    ty, tc = lax.axis_index("ty"), lax.axis_index("tc")
    tp = ty * 2 + tc
    weights = (wqkv, wo, wg, wu, wd)

    def at_x(k):
        return {"fx": lax.rem(fx + k, 4)}

    def at_z(k):
        whole = lax.rem(rep * 4 + fz + k + 8, 8)
        return {"rep": whole // 4, "fz": lax.rem(whole, 4)}

    def at_y(k):
        return {"ty": lax.rem(ty + k, 4)}

    other = {"tc": 1 - tc}

    mine = [
        pltpu.make_async_copy(tokens_hbm, tok, loc_sem.at[0]),
        pltpu.make_async_copy(wq_hbm, wqkv.at[fz, fx, :, :, pl.ds(0, 128)], loc_sem.at[1]),
        pltpu.make_async_copy(wk_hbm, wqkv.at[fz, fx, :, :, pl.ds(128, 128)], loc_sem.at[2]),
        pltpu.make_async_copy(wv_hbm, wqkv.at[fz, fx, :, :, pl.ds(256, 256)], loc_sem.at[3]),
        pltpu.make_async_copy(wo_hbm, wo.at[fz, fx], loc_sem.at[4]),
        pltpu.make_async_copy(wg_hbm, wg.at[fz, fx], loc_sem.at[5]),
        pltpu.make_async_copy(wu_hbm, wu.at[fz, fx], loc_sem.at[6]),
        pltpu.make_async_copy(wd_hbm, wd.at[fz, fx], loc_sem.at[7]),
        pltpu.make_async_copy(shift_hbm, shift, loc_sem.at[8]),
    ]
    for copy in mine:
        copy.start()

    barrier = pltpu.get_barrier_semaphore()
    peers = [at_x(1), at_x(2), at_x(3), at_z(1), at_z(-1), at_z(2), at_z(-2), at_y(1), at_y(2), at_y(3), other]
    for peer in peers:
        pl.semaphore_signal(barrier, inc=1, device_id=peer, device_id_type=MESH)

    mine[0].wait()
    n1[ty, tc] = rms_norm(tok[...].astype(F32), mix_gain[...]).astype(BF16)
    for copy in mine[1:8]:
        copy.wait()

    pl.semaphore_wait(barrier, len(peers))

    pending = []

    def push(src, dst, send, recv, peer):
        copy = pltpu.make_async_remote_copy(
            src_ref=src, dst_ref=dst, send_sem=send, recv_sem=recv, device_id=peer, device_id_type=MESH
        )
        copy.start()
        return copy

    def spread(buf, z, x, first, count, g, phase, peer):
        piece = buf.at[z, x, pl.ds(first, count)]
        push(piece, piece, w_send.at[g, phase], w_recv.at[g, phase], peer)

    def first_phase(g):
        buf = weights[g]
        for k in (1, 3, 2):
            spread(buf, fz, fx, 0, 2, g, 0, at_x(k))
        for k in (1, -1):
            spread(buf, fz, fx, 2, 2, g, 1, at_z(k))
        spread(buf, fz, fx, 2, 1, g, 1, at_z(2))
        spread(buf, fz, fx, 3, 1, g, 1, at_z(-2))

    def three(buf):
        return buf.at[0, pl.ds(0, 3), pl.ds(0, 2)]

    def twelve(buf):
        return buf.at[pl.ds(0, 3), :, pl.ds(0, 2)]

    def await_bytes(view, sem):
        pltpu.make_async_copy(view, view, sem).wait()

    def second_phase(g):
        buf = weights[g]
        await_bytes(three(buf), w_recv.at[g, 0])
        await_bytes(three(buf), w_recv.at[g, 1])
        every = slice(None)
        for k in (1, -1):
            spread(buf, fz, every, 0, 2, g, 2, at_z(k))
        spread(buf, fz, every, 0, 1, g, 2, at_z(2))
        spread(buf, fz, every, 1, 1, g, 2, at_z(-2))
        for k in (1, 3, 2):
            spread(buf, every, fx, 2, 2, g, 3, at_x(k))

    def arrived(g):
        buf = weights[g]
        await_bytes(twelve(buf), w_recv.at[g, 2])
        await_bytes(twelve(buf), w_recv.at[g, 3])

    def gather_start(buf, send, recv):
        own = buf.at[ty, tc]
        for j, peer in enumerate((other, at_y(1), at_y(3), at_y(2))):
            push(own, own, send.at[j], recv.at[tp], peer)

    def gather_next(buf, send, recv, i):
        chip = lax.rem(ty + order(i), 4)
        mine_slot, theirs = buf.at[chip, tc], buf.at[chip, 1 - tc]

        @pl.when(i > 0)
        def _():
            await_bytes(mine_slot, recv.at[chip * 2 + tc])
            push(mine_slot, mine_slot, send.at[3 + i], recv.at[chip * 2 + tc], other)

        await_bytes(theirs, recv.at[chip * 2 + 1 - tc])
        return chip

    def gather_finish(buf, send):
        for j in range(7):
            await_bytes(buf.at[0, 0], send.at[j])

    def cross_start(chip, parts, send_buf, cross_buf, send, recv):
        push(send_buf.at[chip], cross_buf.at[chip], send.at[chip], recv.at[chip], other)

    def scatter_send(chip, keep, cross_buf, recv_buf, x_recv, r_send, r_recv):
        await_bytes(cross_buf.at[chip], x_recv.at[chip])
        keep[chip] = (keep[chip].astype(F32) + cross_buf[chip].astype(F32)).astype(BF16)
        push(keep.at[chip], recv_buf.at[ty], r_send.at[chip], r_recv.at[ty], {"ty": chip})

    gather_start(n1, ag1_send, ag1_recv)
    first_phase(QKV)
    first_phase(OUT)
    first_phase(GATE)
    second_phase(QKV)
    second_phase(OUT)
    first_phase(UP)
    first_phase(DOWN)

    mine[8].wait()

    arrived(QKV)

    @pl.loop(0, 4)
    def project(i):
        chip = gather_next(n1, ag1_send, ag1_recv, i)
        rows = pl.ds(pl.multiple_of(chip * 256, 256), 256)
        x = n1[chip].reshape(256, 2048)
        both = dot(x, wqkv[:, :, :, :, pl.ds(0, 256)].reshape(2048, 256))
        qs[rows, :] = both[:, :128].astype(BF16)
        ks[rows, :] = both[:, 128:].astype(BF16)
        vs[rows, :] = dot(x, wqkv[:, :, :, :, pl.ds(256, 256)].reshape(2048, 256)).astype(BF16)
        low = dot(x, down_proj[...]).astype(BF16)
        cols = pl.ds(pl.multiple_of(tp * 128, 128), 128)
        pre = dot(low, up_proj[:, cols]) + bias[:, cols]
        soft = jnp.minimum(pre, 0.0) - jnp.log1p(jnp.exp(-jnp.abs(pre)))
        shift[rows, :] = soft / TAU + shift[rows, :]

    second_phase(GATE)

    ri = lax.broadcasted_iota(jnp.int32, (128, 128), 0)
    ci = lax.broadcasted_iota(jnp.int32, (128, 128), 1)
    causal = jnp.where((ri >= ci) & (ri // BLK == ci // BLK), 1.0, 0.0).astype(F32)
    state[...] = jnp.zeros_like(state)
    gain_row = head_gain[:, pl.ds(pl.multiple_of(tp * DV, DV), DV)]

    @pl.loop(0, 8)
    def attend(i):
        rows = pl.ds(pl.multiple_of(i * 128, 128), 128)
        cum = lax.dot_general(
            causal, shift[rows, :], (((1,), (0,)), ((), ())),
            preferred_element_type=F32, precision=lax.Precision.HIGHEST,
        )
        v = vs[rows, :]
        k = ks[rows, :].astype(F32)
        q_dec = (qs[rows, :].astype(F32) * KEY_CHANNELS ** (-0.5) * jnp.exp(cum)).astype(BF16)
        k_dec = (k * jnp.exp(-cum)).astype(BF16)
        scores = dot(q_dec, k_dec, (((1,), (1,)), ((), ())))
        scores = jnp.where(causal > 0.5, scores, 0.0).astype(BF16)
        inner = dot(scores, v)
        s = state[...]
        carried = []
        for b in range(2):
            part = slice(b * BLK, (b + 1) * BLK)
            tot = cum[(b + 1) * BLK - 1 : (b + 1) * BLK, :]
            carried.append(dot(q_dec[part], s.astype(BF16), (((1,), (1,)), ((), ()))))
            weighted = (k[part] * jnp.exp(tot - cum[part])).astype(BF16)
            s = jnp.exp(tot) * s + dot(v[part], weighted, (((0,), (0,)), ((), ())))
        state[...] = s
        head = inner + jnp.concatenate(carried, axis=0)
        gated[rows, :] = rms_norm(head, gain_row).astype(BF16)

    second_phase(UP)
    second_phase(DOWN)
    arrived(OUT)

    def col_pair(buf, f):
        left, right = buf[f // 4, f % 4], buf[f // 4, f % 4 + 1]
        depth = left.shape[0] * left.shape[1]
        return jnp.concatenate([left.reshape(depth, 128), right.reshape(depth, 128)], axis=1)

    def partial_out(chip, x, buf, keep, send_buf):
        for f in range(0, 16, 2):
            cols = slice(f * 128, f * 128 + 256)
            part = dot(x, col_pair(buf, f)).astype(BF16)
            keep_it = jnp.where(tc == 0, part[:128], part[128:])
            give_it = jnp.where(tc == 0, part[128:], part[:128])
            keep[chip, :, cols] = keep_it
            send_buf[chip, :, cols] = give_it

    @pl.loop(0, 4)
    def mix(i):
        chip = lax.rem(ty + 2 + i, 4)
        x = gated[pl.ds(pl.multiple_of(chip * 256, 256), 256), :]
        partial_out(chip, x, wo, keep1, send1)
        push(send1.at[chip], cross1.at[chip], x1_send.at[chip], x1_recv.at[chip], other)

    @pl.loop(0, 4)
    def scatter1(i):
        chip = lax.rem(ty + jnp.where(i == 0, 2, jnp.where(i == 1, 1, jnp.where(i == 2, 3, 0))), 4)
        await_bytes(cross1.at[chip], x1_recv.at[chip])

        @pl.when(i < 3)
        def _():
            keep1[chip] = (keep1[chip].astype(F32) + cross1[chip].astype(F32)).astype(BF16)
            push(keep1.at[chip], recv1.at[ty], r1_send.at[chip], r1_recv.at[ty], {"ty": chip})

    hidden[...] = tok[...].astype(F32) + (keep1[ty].astype(F32) + cross1[ty].astype(F32))
    for k in (1, 3, 2):
        chip = lax.rem(ty + k, 4)
        await_bytes(recv1.at[chip], r1_recv.at[chip])
        hidden[...] = hidden[...] + recv1[chip].astype(F32)

    n2[ty, tc] = rms_norm(hidden[...], ffn_gain[...]).astype(BF16)
    gather_start(n2, ag2_send, ag2_recv)
    arrived(GATE)
    arrived(UP)
    arrived(DOWN)

    def finish_chunk(chip):
        await_bytes(cross2.at[chip], x2_recv.at[chip])
        keep2[chip] = (keep2[chip].astype(F32) + cross2[chip].astype(F32)).astype(BF16)
        push(keep2.at[chip], recv2.at[ty], r2_send.at[chip], r2_recv.at[ty], {"ty": chip})

    @pl.loop(0, 4)
    def feed(i):
        chip = gather_next(n2, ag2_send, ag2_recv, i)
        x = n2[chip].reshape(256, 2048)
        for lo, width in ((0, 256), (256, 256), (512, 192)):
            g = dot(x, wg[:, :, :, :, pl.ds(lo, width)].reshape(2048, width))
            u = dot(x, wu[:, :, :, :, pl.ds(lo, width)].reshape(2048, width))
            act[:, pl.ds(lo, width)] = (g * (1.0 / (1.0 + jnp.exp(-g))) * u).astype(BF16)
        partial_out(chip, act[...], wd, keep2, send2)
        push(send2.at[chip], cross2.at[chip], x2_send.at[chip], x2_recv.at[chip], other)

        @pl.when(i > 1)
        def _():
            finish_chunk(lax.rem(ty + order(i - 1), 4))

    finish_chunk(lax.rem(ty + 2, 4))
    await_bytes(cross2.at[ty], x2_recv.at[ty])
    hidden[...] = hidden[...] + (keep2[ty].astype(F32) + cross2[ty].astype(F32))
    total = hidden[...]
    for k in (1, 3, 2):
        chip = lax.rem(ty + k, 4)
        await_bytes(recv2.at[chip], r2_recv.at[chip])
        total = total + recv2[chip].astype(F32)
    out[...] = total

    for g in range(5):
        for phase, view in ((0, three), (1, three), (2, twelve), (3, twelve)):
            await_bytes(view(weights[g]), w_send.at[g, phase])
    gather_finish(n1, ag1_send)
    gather_finish(n2, ag2_send)
    for chip in range(4):
        await_bytes(send1.at[chip], x1_send.at[chip])
        await_bytes(send2.at[chip], x2_send.at[chip])
    for k in range(1, 4):
        chip = lax.rem(ty + k, 4)
        await_bytes(keep1.at[chip], r1_send.at[chip])
        await_bytes(keep2.at[chip], r2_send.at[chip])


def per_device(
    tokens, mix_gain, w_query, w_key, w_value, w_decay_down, w_decay_up, decay_bias, decay_shift,
    head_gain, w_mix_out, ffn_gain, w_gate, w_up, w_down,
):
    any_space = pl.BlockSpec(memory_space=pl.ANY)
    vmem = pl.BlockSpec(memory_space=pltpu.VMEM)
    dma = pltpu.SemaphoreType.DMA
    rows = [pltpu.VMEM((4, 128, 2048), BF16)] * 8
    return pl.pallas_call(
        kernel,
        out_shape=jax.ShapeDtypeStruct((128, 2048), F32),
        in_specs=[any_space] * 9 + [vmem] * 6,
        out_specs=vmem,
        scratch_shapes=[
            pltpu.VMEM((4, 4, 4, 32, 512), BF16),
            pltpu.VMEM((4, 4, 4, 64, 128), BF16),
            pltpu.VMEM((4, 4, 4, 32, 704), BF16),
            pltpu.VMEM((4, 4, 4, 32, 704), BF16),
            pltpu.VMEM((4, 4, 4, 176, 128), BF16),
            pltpu.VMEM((128, 2048), BF16),
            pltpu.VMEM((1024, 128), F32),
            pltpu.VMEM((4, 2, 128, 2048), BF16),
            pltpu.VMEM((4, 2, 128, 2048), BF16),
            pltpu.VMEM((1024, 128), BF16),
            pltpu.VMEM((1024, 128), BF16),
            pltpu.VMEM((1024, 256), BF16),
            pltpu.VMEM((1024, 256), BF16),
            pltpu.VMEM((256, 128), F32),
            pltpu.VMEM((128, 2048), F32),
            pltpu.VMEM((256, 704), BF16),
            *rows,
            dma((9,)), dma((5, 4)), dma((5, 4)),
            dma((7,)), dma((8,)), dma((7,)), dma((8,)),
            *([dma((4,))] * 8),
        ],
        compiler_params=pltpu.CompilerParams(
            collective_id=0, has_side_effects=True, vmem_limit_bytes=60 * 1024 * 1024
        ),
    )(
        tokens,
        decay_shift,
        w_query.reshape(4, 32, 128),
        w_key.reshape(4, 32, 128),
        w_value.reshape(4, 32, 256),
        w_mix_out.reshape(4, 64, 128),
        w_gate.reshape(4, 32, 704),
        w_up.reshape(4, 32, 704),
        w_down.reshape(4, 176, 128),
        mix_gain.reshape(1, -1),
        ffn_gain.reshape(1, -1),
        head_gain.reshape(1, -1),
        w_decay_down,
        w_decay_up,
        decay_bias.reshape(1, -1),
    )


def solution(mesh):
    finer = Mesh(mesh.devices.reshape(mesh.shape["rep"], 4, 4, 4, 2), AXES)
    everything, fs, tp = AXES, ("fz", "fx"), ("ty", "tc")
    return jax.shard_map(
        per_device,
        mesh=finer,
        in_specs=(
            P(everything, None), P(), P(fs, tp), P(fs, tp), P(fs, tp), P(), P(), P(),
            P(("rep", *fs), tp), P(), P(tp, fs), P(), P(fs, tp), P(fs, tp), P(tp, fs),
        ),
        out_specs=P(everything, None),
        check_vma=False,
    )
```

```python
import jax
import jax.numpy as jnp
from jax import lax
from jax.experimental import pallas as pl
from jax.experimental.pallas import tpu as pltpu
from jax.sharding import Mesh
from jax.sharding import PartitionSpec as P

AXES = ("rep", "fz", "fx", "ty", "tc")
MESH = pl.DeviceIdType.MESH
KEY_CHANNELS = 128
DV = 256
BLK = 64
EPS = 1e-06
TAU = 16.0
F32 = jnp.float32
BF16 = jnp.bfloat16
NT = (((1,), (1,)), ((), ()))
TN = (((0,), (0,)), ((), ()))
QKV, OUT, GU0, GU1, DOWN = range(5)
QUARTERS = ((32, 512), (64, 128), (32, 768), (32, 640), (176, 128))


def rms_norm(values, gain):
    return values * lax.rsqrt(jnp.mean(values * values, axis=-1, keepdims=True) + EPS) * gain


def dot(a, b, dims=(((1,), (0,)), ((), ()))):
    return lax.dot_general(a, b, dims, preferred_element_type=F32)


def kernel(
    tokens_hbm, shift_hbm, wq_hbm, wk_hbm, wv_hbm, wo_hbm, wg_hbm, wu_hbm, wd_hbm,
    mix_gain, ffn_gain, head_gain, down_proj, up_proj, bias,
    out,
    wqkv, wo, wgu0, wgu1, wd, gate_t, up_t,
    tok, shift, n1, n2, qs, ks, vs, gated, state, hidden, act,
    part1, cross1, fold1, recv1, part2, cross2, fold2, recv2,
    loc_sem, w_send, w_recv,
    ag1_send, ag1_recv, ag2_send, ag2_recv,
    x1_send, x1_recv, r1_send, r1_recv, x2_send, x2_recv, r2_send, r2_recv,
):
    rep, fz, fx = lax.axis_index("rep"), lax.axis_index("fz"), lax.axis_index("fx")
    ty, tc = lax.axis_index("ty"), lax.axis_index("tc")
    tp = ty * 2 + tc
    weights = (wqkv, wo, wgu0, wgu1, wd)
    every = slice(None)

    def at_x(k):
        return {"fx": lax.rem(fx + k + 4, 4)}

    def at_z(k):
        whole = lax.rem(rep * 4 + fz + k + 8, 8)
        return {"rep": whole // 4, "fz": lax.rem(whole, 4)}

    def at_y(k):
        return {"ty": lax.rem(ty + k + 4, 4)}

    def chip_at(k):
        return lax.rem(ty + k + 4, 4)

    other = {"tc": 1 - tc}

    mine = [
        pltpu.make_async_copy(tokens_hbm, tok, loc_sem.at[0]),
        pltpu.make_async_copy(wq_hbm, wqkv.at[fz, fx, :, :, pl.ds(0, 128)], loc_sem.at[1]),
        pltpu.make_async_copy(wk_hbm, wqkv.at[fz, fx, :, :, pl.ds(128, 128)], loc_sem.at[2]),
        pltpu.make_async_copy(wv_hbm, wqkv.at[fz, fx, :, :, pl.ds(256, 256)], loc_sem.at[3]),
        pltpu.make_async_copy(wo_hbm, wo.at[fz, fx], loc_sem.at[4]),
        pltpu.make_async_copy(wg_hbm, gate_t, loc_sem.at[5]),
        pltpu.make_async_copy(wu_hbm, up_t, loc_sem.at[6]),
        pltpu.make_async_copy(wd_hbm, wd.at[fz, fx], loc_sem.at[7]),
        pltpu.make_async_copy(shift_hbm, shift, loc_sem.at[8]),
    ]
    for copy in mine:
        copy.start()

    barrier = pltpu.get_barrier_semaphore()
    peers = [at_x(1), at_x(2), at_x(3), at_z(1), at_z(-1), at_z(2), at_z(-2), at_y(1), at_y(3), other]
    for peer in peers:
        pl.semaphore_signal(barrier, inc=1, device_id=peer, device_id_type=MESH)

    mine[0].wait()
    normed = rms_norm(tok[...].astype(F32), mix_gain[...]).astype(BF16)
    n1[ty, tc] = normed.reshape(2, 64, 2048)
    for copy in mine[1:8]:
        copy.wait()

    pl.semaphore_wait(barrier, len(peers))

    def push(src, dst, send, recv, peer):
        pltpu.make_async_remote_copy(
            src_ref=src, dst_ref=dst, send_sem=send, recv_sem=recv, device_id=peer, device_id_type=MESH
        ).start()

    def await_bytes(view, sem):
        pltpu.make_async_copy(view, view, sem).wait()

    def spread(g, phase, z, x, first, count, peer):
        piece = weights[g].at[z, x, pl.ds(first, count)]
        push(piece, piece, w_send.at[g, phase], w_recv.at[g, phase], peer)

    def halves(g, phase):
        buf = weights[g]
        if phase < 2:
            return buf.at[0, pl.ds(0, 3), pl.ds(0, 2)]
        if phase < 4:
            return buf.at[pl.ds(0, 2), :, pl.ds(0, 2)]
        return buf.at[0, :, pl.ds(0, 2)]

    def landed(g, *phases):
        for phase in phases:
            await_bytes(halves(g, phase), w_recv.at[g, phase])

    def first_phase(g):
        for k in (1, -1, 2):
            spread(g, 0, fz, fx, 0, 2, at_x(k))
        for k in (1, -1):
            spread(g, 1, fz, fx, 2, 2, at_z(k))
        spread(g, 1, fz, fx, 2, 1, at_z(2))
        spread(g, 1, fz, fx, 3, 1, at_z(-2))

    def second_phase(g):
        landed(g, 0, 1)
        for k in (1, -1):
            spread(g, 2, fz, every, 0, 2, at_z(k))
            spread(g, 3, every, fx, 2, 2, at_x(k))

    def third_phase(g):
        landed(g, 2, 3)
        spread(g, 4, lax.rem(fz + 3, 4), every, 0, 1, at_z(1))
        spread(g, 4, lax.rem(fz + 1, 4), every, 1, 1, at_z(-1))
        spread(g, 5, every, lax.rem(fx + 3, 4), 2, 1, at_x(1))
        spread(g, 5, every, lax.rem(fx + 1, 4), 3, 1, at_x(-1))

    def complete(g):
        landed(g, 4, 5)

    class Gather:
        def __init__(self, buf, send, recv):
            self.buf, self.send, self.recv = buf, send, recv

        def some(self, j, chip, core, h, first, count, peer):
            piece = self.buf.at[chip, core, h, pl.ds(first, count)]
            push(piece, piece, self.send.at[j], self.recv.at[chip, core, h], peer)

        def half(self, j, chip, core, h, peer):
            self.some(j, chip, core, h, 0, 64, peer)

        def came(self, chip, core, h):
            await_bytes(self.buf.at[chip, core, h], self.recv.at[chip, core, h])

        def start(self):
            self.half(0, ty, tc, 0, at_y(1))
            self.half(1, ty, tc, 1, at_y(-1))
            self.half(2, ty, tc, 0, other)
            self.half(3, ty, tc, 1, other)
            self.some(4, ty, tc, 1, 0, 32, at_y(1))
            self.some(5, ty, tc, 0, 0, 32, at_y(-1))

        def step1(self):
            back, ahead = chip_at(-1), chip_at(1)
            self.came(back, tc, 0)
            self.half(6, back, tc, 0, at_y(1))
            self.some(14, ty, tc, 1, 32, 32, at_y(1))
            self.half(7, back, tc, 0, other)
            self.came(ahead, tc, 1)
            self.half(8, ahead, tc, 1, at_y(-1))
            self.some(15, ty, tc, 0, 32, 32, at_y(-1))
            self.half(9, ahead, tc, 1, other)

        def step2(self):
            far = chip_at(2)
            self.came(far, tc, 0)
            self.half(12, far, tc, 0, other)
            self.came(far, tc, 1)
            self.half(13, far, tc, 1, other)

        def step3(self):
            back, ahead = chip_at(-1), chip_at(1)
            self.came(back, tc, 1)
            self.half(10, back, tc, 1, other)
            self.came(ahead, tc, 0)
            self.half(11, ahead, tc, 0, other)

        def theirs(self, chip):
            self.came(chip, 1 - tc, 0)
            self.came(chip, 1 - tc, 1)

        def drain(self):
            for j in (0, 1, 2, 3, 6, 7, 8, 9, 10, 11, 12, 13):
                await_bytes(self.buf.at[0, 0, 0], self.send.at[j])
            for j in (4, 5, 14, 15):
                await_bytes(self.buf.at[0, 0, 0, pl.ds(0, 32)], self.send.at[j])

    class Scatter:
        def __init__(self, part, cross, fold, recv, x_send, x_recv, r_send, r_recv):
            self.part, self.cross, self.fold, self.recv = part, cross, fold, recv
            self.x_send, self.x_recv, self.r_send, self.r_recv = x_send, x_recv, r_send, r_recv

        def swap(self, chip, h):
            push(
                self.part.at[chip, 1 - tc, h], self.cross.at[chip, h],
                self.x_send.at[chip, h], self.x_recv.at[chip, h], other,
            )

        def both(self, chip, h):
            await_bytes(self.cross.at[chip, h], self.x_recv.at[chip, h])
            return self.part[chip, tc, h].astype(F32) + self.cross[chip, h].astype(F32)

        def send(self, j, chip, h, dst, k):
            push(self.part.at[chip, tc, h], dst, self.r_send.at[j], self.r_recv.at[j], at_y(k))

        def far(self):
            chip = chip_at(2)
            for h, k in ((0, 1), (1, -1)):
                self.part[chip, tc, h] = self.both(chip, h).astype(BF16)
                self.send(h, chip, h, self.fold.at[h], k)

        def near(self):
            for d, h, k in ((0, 1, 1), (1, 0, -1)):
                chip = chip_at(k)
                self.part[chip, tc, h] = self.both(chip, h).astype(BF16)
                self.send(2 + d, chip, h, self.recv.at[d, h], k)

        def ready(self):
            for h, k in ((0, 1), (1, -1)):
                chip = chip_at(k)
                self.part[chip, tc, h] = self.both(chip, h).astype(BF16)

        def through(self):
            for d, h, k in ((0, 0, 1), (1, 1, -1)):
                chip = chip_at(k)
                await_bytes(self.fold.at[d], self.r_recv.at[d])
                whole = self.part[chip, tc, h].astype(F32) + self.fold[d].astype(F32)
                self.part[chip, tc, h] = whole.astype(BF16)
                self.send(4 + d, chip, h, self.recv.at[d, h], k)

        def own(self):
            return jnp.concatenate([self.both(ty, 0), self.both(ty, 1)], axis=0)

        def total(self):
            for j in range(2, 6):
                await_bytes(self.fold.at[0], self.r_recv.at[j])
            return (self.recv[0].astype(F32) + self.recv[1].astype(F32)).reshape(128, 2048)

        def drain(self):
            for chip in range(4):
                for h in range(2):
                    await_bytes(self.cross.at[chip, h], self.x_send.at[chip, h])
            for j in range(6):
                await_bytes(self.fold.at[0], self.r_send.at[j])

    gather1 = Gather(n1, ag1_send, ag1_recv)
    gather2 = Gather(n2, ag2_send, ag2_recv)
    scatter1 = Scatter(part1, cross1, fold1, recv1, x1_send, x1_recv, r1_send, r1_recv)
    scatter2 = Scatter(part2, cross2, fold2, recv2, x2_send, x2_recv, r2_send, r2_recv)

    with jax.named_scope("start"):
        gather1.start()
        first_phase(QKV)

    with jax.named_scope("turn"):
        def turned(ref, first):
            return ref[pl.ds(first, 256), :].T.reshape(4, 32, 256)

        def mixed(first, count):
            both = jnp.concatenate([gate_t[pl.ds(first, count), :], up_t[pl.ds(first, count), :]], axis=0)
            return both.T.reshape(4, 32, 2 * count)

        wgu0[fz, fx, :, :, 0:256] = turned(gate_t, 0)
        wgu0[fz, fx, :, :, 256:512] = turned(up_t, 0)
        wgu0[fz, fx, :, :, 512:768] = mixed(512, 128)
        wgu1[fz, fx, :, :, 0:256] = turned(gate_t, 256)
        wgu1[fz, fx, :, :, 256:512] = turned(up_t, 256)
        wgu1[fz, fx, :, :, 512:640] = mixed(640, 64)

    with jax.named_scope("second_qkv"):
        second_phase(QKV)
        first_phase(OUT)
    with jax.named_scope("ag1_step1"):
        gather1.step1()
    with jax.named_scope("third_qkv"):
        third_phase(QKV)
    with jax.named_scope("second_out"):
        second_phase(OUT)
        first_phase(GU0)
        first_phase(GU1)
    with jax.named_scope("ag1_step2"):
        gather1.step2()
        mine[8].wait()
        gather1.theirs(ty)
    with jax.named_scope("complete_qkv"):
        complete(QKV)

    @pl.loop(0, 4)
    def project(i):
        chip = chip_at(jnp.where(i == 0, 0, jnp.where(i == 1, 2, jnp.where(i == 2, 1, 3))))
        with jax.named_scope("project_wait"):
            @pl.when(i == 2)
            def _():
                gather1.step3()

            @pl.when(i > 0)
            def _():
                gather1.theirs(chip)

        with jax.named_scope("project"):
            rows = pl.ds(pl.multiple_of(chip * 256, 256), 256)
            x = n1[chip].reshape(256, 2048)
            both = dot(x, wqkv[:, :, :, :, pl.ds(0, 256)].reshape(2048, 256))
            qs[rows, :] = both[:, :128].astype(BF16)
            ks[rows, :] = both[:, 128:].astype(BF16)
            vs[rows, :] = dot(x, wqkv[:, :, :, :, pl.ds(256, 256)].reshape(2048, 256)).astype(BF16)
            low = dot(x, down_proj[...], NT).astype(BF16)
            cols = pl.ds(pl.multiple_of(tp * 128, 128), 128)
            pre = dot(low, up_proj[:, cols]) + bias[:, cols]
            soft = jnp.minimum(pre, 0.0) - jnp.log1p(jnp.exp(-jnp.abs(pre)))
            shift[rows, :] = soft / TAU + shift[rows, :]

    with jax.named_scope("third_out_second_gu0"):
        third_phase(OUT)
        second_phase(GU0)

    ri = lax.broadcasted_iota(jnp.int32, (128, 128), 0)
    ci = lax.broadcasted_iota(jnp.int32, (128, 128), 1)
    causal = jnp.where((ri >= ci) & (ri // BLK == ci // BLK), 1.0, 0.0).astype(F32)
    state[...] = jnp.zeros_like(state)
    gain_row = head_gain[:, pl.ds(pl.multiple_of(tp * DV, DV), DV)]

    @pl.loop(0, 8, unroll=2)
    def attend(i):
        with jax.named_scope("attend"):
            rows = pl.ds(pl.multiple_of(i * 128, 128), 128)
            cum = lax.dot_general(
                causal, shift[rows, :], (((1,), (0,)), ((), ())),
                preferred_element_type=F32, precision=lax.Precision.HIGHEST,
            )
            v = vs[rows, :]
            k = ks[rows, :].astype(F32)
            q_dec = (qs[rows, :].astype(F32) * KEY_CHANNELS ** (-0.5) * jnp.exp(cum)).astype(BF16)
            k_dec = (k * jnp.exp(-cum)).astype(BF16)
            scores = dot(q_dec, k_dec, NT)
            scores = jnp.where(causal > 0.5, scores, 0.0).astype(BF16)
            inner = dot(scores, v)
            s = state[...]
            carried = []
            for b in range(2):
                part = slice(b * BLK, (b + 1) * BLK)
                tot = cum[(b + 1) * BLK - 1 : (b + 1) * BLK, :]
                carried.append(dot(q_dec[part], s.astype(BF16), NT))
                weighted = (k[part] * jnp.exp(tot - cum[part])).astype(BF16)
                s = jnp.exp(tot) * s + dot(v[part], weighted, TN)
            state[...] = s
            head = inner + jnp.concatenate(carried, axis=0)
            gated[rows, :] = rms_norm(head, gain_row).astype(BF16)

    with jax.named_scope("second_gu1"):
        second_phase(GU1)
        first_phase(DOWN)
    with jax.named_scope("complete_out"):
        complete(OUT)

    def partial_out(x, buf, scatter, places):
        for f in range(0, 16, 2):
            left, right = buf[f // 4, f % 4], buf[f // 4, f % 4 + 1]
            depth = left.shape[0] * left.shape[1]
            w = jnp.concatenate([left.reshape(depth, 128), right.reshape(depth, 128)], axis=1)
            product = dot(x, w).astype(BF16)
            for p, (chip, core, h) in enumerate(places):
                scatter.part[chip, core, h, :, f * 128 : f * 128 + 256] = product[p * 64 : p * 64 + 64]
        for chip, core, h in places:
            if core == 0:
                scatter.swap(chip, h)

    def whole_chip(chip):
        return [(chip, 0, 0), (chip, 0, 1), (chip, 1, 0), (chip, 1, 1)]

    def by_halves(chip):
        return [(chip, 0, 0), (chip, 1, 0), (chip, 0, 1), (chip, 1, 1)]

    def two_halves(h_back):
        back, ahead = chip_at(-1), chip_at(1)
        return [(back, 0, h_back), (back, 1, h_back), (ahead, 0, 1 - h_back), (ahead, 1, 1 - h_back)]

    @pl.loop(0, 4)
    def mix(i):
        with jax.named_scope("mix"):
            chip = chip_at(jnp.where(i == 0, 2, jnp.where(i == 1, 1, jnp.where(i == 2, 3, 0))))
            x = gated[pl.ds(pl.multiple_of(chip * 256, 256), 256), :]
            partial_out(x, wo, scatter1, whole_chip(chip))

    with jax.named_scope("rs1_far"):
        scatter1.far()
    with jax.named_scope("rs1_near"):
        scatter1.near()
        scatter1.ready()
        hidden[...] = tok[...].astype(F32) + scatter1.own()
    with jax.named_scope("third_gu0"):
        third_phase(GU0)
    with jax.named_scope("rs1_through"):
        scatter1.through()
    with jax.named_scope("third_gu1"):
        third_phase(GU1)
    with jax.named_scope("second_down"):
        second_phase(DOWN)
    with jax.named_scope("rs1_total"):
        hidden[...] = hidden[...] + scatter1.total()
    with jax.named_scope("norm2"):
        n2[ty, tc] = rms_norm(hidden[...], ffn_gain[...]).astype(BF16).reshape(2, 64, 2048)
        gather2.start()

    def gate_up(slot, x):
        def product(buf, first, width):
            return dot(x, buf[:, :, :, :, pl.ds(first, width)].reshape(2048, width))

        def gate(g, u):
            return (g * (1.0 / (1.0 + jnp.exp(-g))) * u).astype(BF16)

        act[slot, :, 0:256] = gate(product(wgu0, 0, 256), product(wgu0, 256, 256))
        act[slot, :, 256:512] = gate(product(wgu1, 0, 256), product(wgu1, 256, 256))
        both = product(wgu0, 512, 256)
        act[slot, :, 512:640] = gate(both[:, :128], both[:, 128:])
        both = product(wgu1, 512, 128)
        act[slot, :, 640:704] = gate(both, pltpu.roll(both, 64, 1))[:, :64]

    @pl.loop(0, 4)
    def feed(i):
        with jax.named_scope("feed_wait"):
            @pl.when(i == 0)
            def _():
                gather2.theirs(ty)
                gather2.step1()
                complete(GU0)
                complete(GU1)

            @pl.when(i == 1)
            def _():
                third_phase(DOWN)
                gather2.came(chip_at(-1), 1 - tc, 0)
                gather2.came(chip_at(1), 1 - tc, 1)
                gather2.step2()

            @pl.when(i == 2)
            def _():
                gather2.theirs(chip_at(2))

        with jax.named_scope("rs2_adds"):
            @pl.when(i == 3)
            def _():
                complete(DOWN)
                partial_out(act[2], wd, scatter2, by_halves(chip_at(2)))
                gather2.step3()
                partial_out(act[1], wd, scatter2, two_halves(0))
                scatter2.far()
                gather2.came(chip_at(-1), 1 - tc, 1)
                gather2.came(chip_at(1), 1 - tc, 0)

        with jax.named_scope("gate_up"):
            chip_a = chip_at(jnp.where(i == 0, 0, jnp.where(i == 2, 2, -1)))
            chip_b = chip_at(jnp.where(i == 0, 0, jnp.where(i == 2, 2, 1)))
            h_a = jnp.where(i == 3, 1, 0)
            gate_up(i, jnp.concatenate([n2[chip_a, :, h_a].reshape(128, 2048), n2[chip_b, :, 1 - h_a].reshape(128, 2048)], axis=0))

    with jax.named_scope("rs2_near"):
        scatter2.near()
    with jax.named_scope("down_b"):
        partial_out(act[3], wd, scatter2, two_halves(1))
    with jax.named_scope("down_own"):
        partial_out(act[0], wd, scatter2, by_halves(ty))
    with jax.named_scope("rs2_ready"):
        scatter2.ready()
        hidden[...] = hidden[...] + scatter2.own()
    with jax.named_scope("rs2_through"):
        scatter2.through()
    with jax.named_scope("rs2_total"):
        out[...] = hidden[...] + scatter2.total()

    with jax.named_scope("drain"):
        for g in range(5):
            for phase in range(6):
                await_bytes(halves(g, phase), w_send.at[g, phase])
        gather1.drain()
        gather2.drain()
        scatter1.drain()
        scatter2.drain()


def per_device(
    tokens, mix_gain, w_query, w_key, w_value, w_decay_down, w_decay_up, decay_bias, decay_shift,
    head_gain, w_mix_out, ffn_gain, w_gate, w_up, w_down,
):
    any_space = pl.BlockSpec(memory_space=pl.ANY)
    vmem = pl.BlockSpec(memory_space=pltpu.VMEM)
    dma = pltpu.SemaphoreType.DMA
    scatter = [
        pltpu.VMEM((4, 2, 2, 64, 2048), BF16),
        pltpu.VMEM((4, 2, 64, 2048), BF16),
        pltpu.VMEM((2, 64, 2048), BF16),
        pltpu.VMEM((2, 2, 64, 2048), BF16),
    ]
    return pl.pallas_call(
        kernel,
        out_shape=jax.ShapeDtypeStruct((128, 2048), F32),
        in_specs=[any_space] * 9 + [vmem] * 6,
        out_specs=vmem,
        scratch_shapes=[
            *[pltpu.VMEM((4, 4, 4, *quarter), BF16) for quarter in QUARTERS],
            pltpu.VMEM((704, 128), BF16),
            pltpu.VMEM((704, 128), BF16),
            pltpu.VMEM((128, 2048), BF16),
            pltpu.VMEM((1024, 128), F32),
            pltpu.VMEM((4, 2, 2, 64, 2048), BF16),
            pltpu.VMEM((4, 2, 2, 64, 2048), BF16),
            pltpu.VMEM((1024, 128), BF16),
            pltpu.VMEM((1024, 128), BF16),
            pltpu.VMEM((1024, 256), BF16),
            pltpu.VMEM((1024, 256), BF16),
            pltpu.VMEM((256, 128), F32),
            pltpu.VMEM((128, 2048), F32),
            pltpu.VMEM((4, 256, 704), BF16),
            *scatter, *scatter,
            dma((9,)), dma((5, 6)), dma((5, 6)),
            dma((16,)), dma((4, 2, 2)), dma((16,)), dma((4, 2, 2)),
            dma((4, 2)), dma((4, 2)), dma((6,)), dma((6,)),
            dma((4, 2)), dma((4, 2)), dma((6,)), dma((6,)),
        ],
        compiler_params=pltpu.CompilerParams(
            collective_id=0, has_side_effects=True, vmem_limit_bytes=60 * 1024 * 1024
        ),
    )(
        tokens,
        decay_shift,
        w_query.reshape(4, 32, 128),
        w_key.reshape(4, 32, 128),
        w_value.reshape(4, 32, 256),
        w_mix_out.reshape(4, 64, 128),
        w_gate.T,
        w_up.T,
        w_down.reshape(4, 176, 128),
        mix_gain.reshape(1, -1),
        ffn_gain.reshape(1, -1),
        head_gain.reshape(1, -1),
        w_decay_down.T,
        w_decay_up,
        decay_bias.reshape(1, -1),
    )


def solution(mesh):
    finer = Mesh(mesh.devices.reshape(mesh.shape["rep"], 4, 4, 4, 2), AXES)
    everything, fs, tp = AXES, ("fz", "fx"), ("ty", "tc")
    return jax.shard_map(
        per_device,
        mesh=finer,
        in_specs=(
            P(everything, None), P(), P(fs, tp), P(fs, tp), P(fs, tp), P(), P(), P(),
            P(("rep", *fs), tp), P(), P(tp, fs), P(), P(fs, tp), P(fs, tp), P(tp, fs),
        ),
        out_specs=P(everything, None),
        check_vma=False,
    )
```

```python
import jax
import jax.numpy as jnp
from jax import lax
from jax.experimental import pallas as pl
from jax.experimental.pallas import tpu as pltpu
from jax.sharding import Mesh
from jax.sharding import PartitionSpec as P

AXES = ("rep", "fz", "fx", "ty", "tc")
MESH = pl.DeviceIdType.MESH
KEY_CHANNELS = 128
DV = 256
BLK = 64
EPS = 1e-06
TAU = 16.0
F32 = jnp.float32
BF16 = jnp.bfloat16
NT = (((1,), (1,)), ((), ()))
TN = (((0,), (0,)), ((), ()))
QKV, OUT, GU0, GU1, DOWN = range(5)
QUARTERS = ((32, 512), (64, 128), (32, 768), (32, 640), (176, 128))


def rms_norm(values, gain):
    return values * lax.rsqrt(jnp.mean(values * values, axis=-1, keepdims=True) + EPS) * gain


def dot(a, b, dims=(((1,), (0,)), ((), ()))):
    return lax.dot_general(a, b, dims, preferred_element_type=F32)


def kernel(
    tokens_hbm, shift_hbm, wq_hbm, wk_hbm, wv_hbm, wo_hbm, wg_hbm, wu_hbm, wd_hbm,
    mix_gain, ffn_gain, head_gain, down_proj, up_proj, bias,
    out,
    wqkv, wo, wgu0, wgu1, wd, gate_t, up_t,
    tok, shift, cums, n1, n2, qs, ks, vs, gated, state, hidden, act,
    part1, cross1, fold1, recv1, part2, cross2, fold2, recv2,
    loc_sem, w_send, w_recv,
    ag1_send, ag1_recv, ag2_send, ag2_recv,
    x1_send, x1_recv, r1_send, r1_recv, x2_send, x2_recv, r2_send, r2_recv,
):
    rep, fz, fx = lax.axis_index("rep"), lax.axis_index("fz"), lax.axis_index("fx")
    ty, tc = lax.axis_index("ty"), lax.axis_index("tc")
    tp = ty * 2 + tc
    weights = (wqkv, wo, wgu0, wgu1, wd)
    every = slice(None)

    def at_x(k):
        return {"fx": lax.rem(fx + k + 4, 4)}

    def at_z(k):
        whole = lax.rem(rep * 4 + fz + k + 8, 8)
        return {"rep": whole // 4, "fz": lax.rem(whole, 4)}

    def at_y(k):
        return {"ty": lax.rem(ty + k + 4, 4)}

    def chip_at(k):
        return lax.rem(ty + k + 4, 4)

    other = {"tc": 1 - tc}

    mine = [
        pltpu.make_async_copy(tokens_hbm, tok, loc_sem.at[0]),
        pltpu.make_async_copy(wq_hbm, wqkv.at[fz, fx, :, :, pl.ds(0, 128)], loc_sem.at[1]),
        pltpu.make_async_copy(wk_hbm, wqkv.at[fz, fx, :, :, pl.ds(128, 128)], loc_sem.at[2]),
        pltpu.make_async_copy(wv_hbm, wqkv.at[fz, fx, :, :, pl.ds(256, 256)], loc_sem.at[3]),
        pltpu.make_async_copy(wo_hbm, wo.at[fz, fx], loc_sem.at[4]),
        pltpu.make_async_copy(wg_hbm, gate_t, loc_sem.at[5]),
        pltpu.make_async_copy(wu_hbm, up_t, loc_sem.at[6]),
        pltpu.make_async_copy(wd_hbm, wd.at[fz, fx], loc_sem.at[7]),
        pltpu.make_async_copy(shift_hbm, shift, loc_sem.at[8]),
    ]
    for copy in mine:
        copy.start()

    barrier = pltpu.get_barrier_semaphore()
    peers = [at_x(1), at_x(2), at_x(3), at_z(1), at_z(-1), at_z(2), at_z(-2), at_y(1), at_y(3), other]
    for peer in peers:
        pl.semaphore_signal(barrier, inc=1, device_id=peer, device_id_type=MESH)

    mine[0].wait()
    normed = rms_norm(tok[...].astype(F32), mix_gain[...]).astype(BF16)
    n1[ty, tc] = normed.reshape(2, 64, 2048)
    for copy in mine[1:8]:
        copy.wait()

    pl.semaphore_wait(barrier, len(peers))

    def push(src, dst, send, recv, peer):
        pltpu.make_async_remote_copy(
            src_ref=src, dst_ref=dst, send_sem=send, recv_sem=recv, device_id=peer, device_id_type=MESH
        ).start()

    def await_bytes(view, sem):
        pltpu.make_async_copy(view, view, sem).wait()

    def spread(g, phase, z, x, first, count, peer):
        piece = weights[g].at[z, x, pl.ds(first, count)]
        push(piece, piece, w_send.at[g, phase], w_recv.at[g, phase], peer)

    def halves(g, phase):
        buf = weights[g]
        if phase < 2:
            return buf.at[0, pl.ds(0, 3), pl.ds(0, 2)]
        if phase < 4:
            return buf.at[pl.ds(0, 2), :, pl.ds(0, 2)]
        return buf.at[0, :, pl.ds(0, 2)]

    def landed(g, *phases):
        for phase in phases:
            await_bytes(halves(g, phase), w_recv.at[g, phase])

    def first_phase(g):
        for k in (1, -1, 2):
            spread(g, 0, fz, fx, 0, 2, at_x(k))
        for k in (1, -1):
            spread(g, 1, fz, fx, 2, 2, at_z(k))
        spread(g, 1, fz, fx, 2, 1, at_z(2))
        spread(g, 1, fz, fx, 3, 1, at_z(-2))

    def second_phase(g):
        landed(g, 0, 1)
        for k in (1, -1):
            spread(g, 2, fz, every, 0, 2, at_z(k))
            spread(g, 3, every, fx, 2, 2, at_x(k))

    def third_phase(g):
        landed(g, 2, 3)
        spread(g, 4, lax.rem(fz + 3, 4), every, 0, 1, at_z(1))
        spread(g, 4, lax.rem(fz + 1, 4), every, 1, 1, at_z(-1))
        spread(g, 5, every, lax.rem(fx + 3, 4), 2, 1, at_x(1))
        spread(g, 5, every, lax.rem(fx + 1, 4), 3, 1, at_x(-1))

    def complete(g):
        landed(g, 4, 5)

    class Gather:
        def __init__(self, buf, send, recv):
            self.buf, self.send, self.recv = buf, send, recv

        def some(self, j, chip, core, h, first, count, peer):
            piece = self.buf.at[chip, core, h, pl.ds(first, count)]
            push(piece, piece, self.send.at[j], self.recv.at[chip, core, h], peer)

        def half(self, j, chip, core, h, peer):
            self.some(j, chip, core, h, 0, 64, peer)

        def came(self, chip, core, h):
            await_bytes(self.buf.at[chip, core, h], self.recv.at[chip, core, h])

        def start(self, q):
            rows = pl.ds(q * 32, 32)
            own, ahead, back = self.buf.at[ty, tc], at_y(1), at_y(-1)
            plan = [(0, ahead), (1, back), (0, other), (1, other)]
            for j, (h, peer) in enumerate(plan):
                push(own.at[h, rows], own.at[h, rows], self.send.at[q * 4 + j], self.recv.at[ty, tc, h], peer)
            if q == 1:
                self.some(14, ty, tc, 1, 0, 32, ahead)
                self.some(15, ty, tc, 0, 0, 32, back)

        def step1(self):
            back, ahead = chip_at(-1), chip_at(1)
            self.came(back, tc, 0)
            self.half(8, back, tc, 0, at_y(1))
            self.some(16, ty, tc, 1, 32, 32, at_y(1))
            self.half(9, back, tc, 0, other)
            self.came(ahead, tc, 1)
            self.half(18, ahead, tc, 1, at_y(-1))
            self.some(17, ty, tc, 0, 32, 32, at_y(-1))
            self.half(19, ahead, tc, 1, other)

        def step2(self):
            far = chip_at(2)
            self.came(far, tc, 0)
            self.half(12, far, tc, 0, other)
            self.came(far, tc, 1)
            self.half(13, far, tc, 1, other)

        def step3(self):
            back, ahead = chip_at(-1), chip_at(1)
            self.came(back, tc, 1)
            self.half(10, back, tc, 1, other)
            self.came(ahead, tc, 0)
            self.half(11, ahead, tc, 0, other)

        def theirs(self, chip):
            self.came(chip, 1 - tc, 0)
            self.came(chip, 1 - tc, 1)

        def drain(self):
            for j in range(20):
                whole = j in (8, 9, 10, 11, 12, 13, 18, 19)
                await_bytes(self.buf.at[0, 0, 0, pl.ds(0, 64 if whole else 32)], self.send.at[j])

    class Scatter:
        def __init__(self, part, cross, fold, recv, x_send, x_recv, r_send, r_recv):
            self.part, self.cross, self.fold, self.recv = part, cross, fold, recv
            self.x_send, self.x_recv, self.r_send, self.r_recv = x_send, x_recv, r_send, r_recv

        def swap(self, chip, h):
            push(
                self.part.at[chip, 1 - tc, h], self.cross.at[chip, h],
                self.x_send.at[chip, h], self.x_recv.at[chip, h], other,
            )

        def both(self, chip, h):
            await_bytes(self.cross.at[chip, h], self.x_recv.at[chip, h])
            return self.part[chip, tc, h].astype(F32) + self.cross[chip, h].astype(F32)

        def send(self, j, src, dst, k):
            push(src, dst, self.r_send.at[j], self.r_recv.at[j], at_y(k))

        def far(self):
            chip = chip_at(2)
            for h in range(2):
                self.part[chip, tc, h] = self.both(chip, h).astype(BF16)
            for q in range(2):
                rows = pl.ds(q * 32, 32)
                for h, k in ((0, 1), (1, -1)):
                    self.send(q * 2 + h, self.part.at[chip, tc, h, rows], self.fold.at[h, rows], k)

        def near(self):
            for d, h, k in ((0, 1, 1), (1, 0, -1)):
                chip = chip_at(k)
                self.part[chip, tc, h] = self.both(chip, h).astype(BF16)
                self.send(4 + d, self.part.at[chip, tc, h], self.recv.at[d, h], k)

        def ready(self):
            for h, k in ((0, 1), (1, -1)):
                chip = chip_at(k)
                self.part[chip, tc, h] = self.both(chip, h).astype(BF16)

        def through(self):
            for q in range(2):
                rows = pl.ds(q * 32, 32)
                for d, k in ((0, 1), (1, -1)):
                    chip = chip_at(k)
                    await_bytes(self.fold.at[d, rows], self.r_recv.at[q * 2 + d])
                    whole = self.part[chip, tc, d, rows].astype(F32) + self.fold[d, rows].astype(F32)
                    self.part[chip, tc, d, rows] = whole.astype(BF16)
                    self.send(6 + q * 2 + d, self.part.at[chip, tc, d, rows], self.recv.at[d, d, rows], k)

        def total(self, q):
            rows = pl.ds(q * 32, 32)
            for d in range(2):
                if q == 0:
                    await_bytes(self.recv.at[d, 1 - d], self.r_recv.at[4 + d])
                await_bytes(self.recv.at[d, d, rows], self.r_recv.at[6 + q * 2 + d])
            return self.recv[0, :, rows].astype(F32) + self.recv[1, :, rows].astype(F32)

        def own(self, h):
            return self.both(ty, h)

        def drain(self):
            for chip in range(4):
                for h in range(2):
                    await_bytes(self.cross.at[chip, h], self.x_send.at[chip, h])
            for j in range(10):
                await_bytes(self.fold.at[0, pl.ds(0, 64 if j in (4, 5) else 32)], self.r_send.at[j])

    gather1 = Gather(n1, ag1_send, ag1_recv)
    gather2 = Gather(n2, ag2_send, ag2_recv)
    scatter1 = Scatter(part1, cross1, fold1, recv1, x1_send, x1_recv, r1_send, r1_recv)
    scatter2 = Scatter(part2, cross2, fold2, recv2, x2_send, x2_recv, r2_send, r2_recv)

    with jax.named_scope("start"):
        gather1.start(0)
        gather1.start(1)
        first_phase(QKV)
        first_phase(OUT)

    with jax.named_scope("turn"):
        def turned(ref, first):
            return ref[pl.ds(first, 256), :].T.reshape(4, 32, 256)

        def mixed(first, count):
            both = jnp.concatenate([gate_t[pl.ds(first, count), :], up_t[pl.ds(first, count), :]], axis=0)
            return both.T.reshape(4, 32, 2 * count)

        wgu0[fz, fx, :, :, 0:256] = turned(gate_t, 0)
        wgu0[fz, fx, :, :, 256:512] = turned(up_t, 0)
        wgu0[fz, fx, :, :, 512:768] = mixed(512, 128)
        wgu1[fz, fx, :, :, 0:256] = turned(gate_t, 256)
        wgu1[fz, fx, :, :, 256:512] = turned(up_t, 256)
        wgu1[fz, fx, :, :, 512:640] = mixed(640, 64)

    def row_set(i):
        chip_a = chip_at(jnp.where(i == 0, 0, jnp.where(i == 2, 2, -1)))
        chip_b = chip_at(jnp.where(i == 0, 0, jnp.where(i == 2, 2, 1)))
        h_a = jnp.where(i == 3, 1, 0)
        return [(chip_a, 0, h_a), (chip_a, 1, h_a), (chip_b, 0, 1 - h_a), (chip_b, 1, 1 - h_a)]

    def rows_of(buf, places):
        return jnp.concatenate([buf[place] for place in places], axis=0)

    def from_other(gather, places):
        for chip, _, h in places[::2]:
            gather.came(chip, 1 - tc, h)

    def block(place):
        chip, core, h = place
        return chip * 4 + core * 2 + h

    cols = pl.ds(pl.multiple_of(tp * 128, 128), 128)

    def causal_mask(size, dtype):
        ri = lax.broadcasted_iota(jnp.int32, (size, size), 0)
        ci = lax.broadcasted_iota(jnp.int32, (size, size), 1)
        return jnp.where((ri >= ci) & (ri // BLK == ci // BLK), 1.0, 0.0).astype(dtype)

    def decay(places):
        x = rows_of(n1, places)
        low = dot(x, down_proj[...], NT).astype(BF16)
        pre = dot(low, up_proj[:, cols]) + bias[:, cols]
        soft = jnp.minimum(pre, 0.0) - jnp.log1p(jnp.exp(-jnp.abs(pre)))
        logs = soft / TAU + jnp.concatenate([shift[block(place)] for place in places], axis=0)
        one = logs.astype(BF16)
        rest = logs - one.astype(F32)
        two = rest.astype(BF16)
        three = (rest - two.astype(F32)).astype(BF16)
        sums = dot(causal_mask(256, BF16), jnp.concatenate([one, two, three], axis=1))
        cum = sums[:, :128] + sums[:, 128:256] + sums[:, 256:]
        for p, place in enumerate(places):
            cums[block(place)] = cum[p * 64 : p * 64 + 64]

    with jax.named_scope("second_qkv"):
        second_phase(QKV)
    with jax.named_scope("decay0"):
        mine[8].wait()
        own_set, first_set = row_set(0), row_set(1)
        from_other(gather1, own_set)
        decay(own_set)
    with jax.named_scope("ag1_step1"):
        gather1.step1()
    with jax.named_scope("second_out"):
        second_phase(OUT)
    with jax.named_scope("third_qkv"):
        third_phase(QKV)
        first_phase(GU0)
    with jax.named_scope("decay1"):
        from_other(gather1, first_set)
        decay(first_set)
    with jax.named_scope("ag1_step2"):
        gather1.step2()
    with jax.named_scope("third_out"):
        third_phase(OUT)
        first_phase(GU1)
    with jax.named_scope("complete_qkv"):
        complete(QKV)

    @pl.loop(0, 4)
    def project(i):
        places = row_set(i)
        with jax.named_scope("project_wait"):
            @pl.when(i == 2)
            def _():
                gather1.step3()

        with jax.named_scope("decay"):
            @pl.when(i > 1)
            def _():
                from_other(gather1, places)
                decay(places)

        with jax.named_scope("project"):
            x = rows_of(n1, places)
            both = dot(x, wqkv[:, :, :, :, pl.ds(0, 256)].reshape(2048, 256)).astype(BF16)
            values = dot(x, wqkv[:, :, :, :, pl.ds(256, 256)].reshape(2048, 256)).astype(BF16)
            for p, place in enumerate(places):
                piece = slice(p * 64, p * 64 + 64)
                qs[block(place)] = both[piece, :128]
                ks[block(place)] = both[piece, 128:]
                vs[block(place)] = values[piece]

    with jax.named_scope("second_gu0"):
        second_phase(GU0)
        first_phase(DOWN)

    causal = causal_mask(128, F32)
    state[...] = jnp.zeros_like(state)
    gain_row = head_gain[:, pl.ds(pl.multiple_of(tp * DV, DV), DV)]

    def attend(i):
        pair = pl.ds(i * 2, 2)
        cum = cums[pair].reshape(128, 128)
        v = vs[pair].reshape(128, DV)
        k = ks[pair].reshape(128, 128).astype(F32)
        q_full = qs[pair].reshape(128, 128).astype(F32) * KEY_CHANNELS ** (-0.5) * jnp.exp(cum)
        k_full = k * jnp.exp(-cum)
        q_dec, k_dec = q_full.astype(BF16), k_full.astype(BF16)
        q_low = (q_full - q_dec.astype(F32)).astype(BF16)
        k_low = (k_full - k_dec.astype(F32)).astype(BF16)
        scores = dot(
            jnp.concatenate([q_dec, q_dec, q_low], axis=1),
            jnp.concatenate([k_dec, k_low, k_dec], axis=1), NT,
        )
        scores = jnp.where(causal > 0.5, scores, 0.0).astype(BF16)
        inner = dot(scores, v)
        s = state[...]
        carried = []
        for b in range(2):
            part = slice(b * BLK, (b + 1) * BLK)
            tot = cum[(b + 1) * BLK - 1 : (b + 1) * BLK, :]
            carried.append(dot(q_dec[part], s.astype(BF16), NT))
            weighted = (k[part] * jnp.exp(tot - cum[part])).astype(BF16)
            s = jnp.exp(tot) * s + dot(v[part], weighted, TN)
        state[...] = s
        head = inner + jnp.concatenate(carried, axis=0)
        gated[pair] = rms_norm(head, gain_row).astype(BF16).reshape(2, BLK, DV)

    with jax.named_scope("attend"):
        pl.loop(0, 8, unroll=2)(attend)
    with jax.named_scope("complete_out"):
        complete(OUT)

    def partial_out(x, buf, scatter, places):
        for f in range(0, 16, 2):
            left, right = buf[f // 4, f % 4], buf[f // 4, f % 4 + 1]
            depth = left.shape[0] * left.shape[1]
            w = jnp.concatenate([left.reshape(depth, 128), right.reshape(depth, 128)], axis=1)
            product = dot(x, w).astype(BF16)
            for p, (chip, core, h) in enumerate(places):
                scatter.part[chip, core, h, :, f * 128 : f * 128 + 256] = product[p * 64 : p * 64 + 64]
        for chip, core, h in places:
            if core == 0:
                scatter.swap(chip, h)

    @pl.loop(0, 4)
    def mix(i):
        with jax.named_scope("mix"):
            chip = chip_at(jnp.where(i == 0, 2, jnp.where(i == 1, 1, jnp.where(i == 2, 3, 0))))
            x = gated[pl.ds(chip * 4, 4)].reshape(256, DV)
            partial_out(x, wo, scatter1, [(chip, 0, 0), (chip, 0, 1), (chip, 1, 0), (chip, 1, 1)])

    with jax.named_scope("rs1_far"):
        scatter1.far()
    with jax.named_scope("rs1_near"):
        scatter1.near()
        scatter1.ready()
        for h in range(2):
            own = tok[pl.ds(h * 64, 64), :].astype(F32) + scatter1.own(h)
            hidden[h] = own
    with jax.named_scope("second_gu1"):
        second_phase(GU1)
    with jax.named_scope("rs1_through"):
        scatter1.through()
    with jax.named_scope("third_gu0"):
        third_phase(GU0)
    for q in range(2):
        with jax.named_scope("rs1_total"):
            rows = pl.ds(q * 32, 32)
            values = hidden[:, rows] + scatter1.total(q)
            hidden[:, rows] = values
            n2[ty, tc, :, rows] = rms_norm(values, ffn_gain[...]).astype(BF16)
            gather2.start(q)
    with jax.named_scope("third_gu1"):
        third_phase(GU1)
        second_phase(DOWN)

    def gate_up(slot, x):
        def product(buf, first, width):
            return dot(x, buf[:, :, :, :, pl.ds(first, width)].reshape(2048, width))

        def gate(g, u):
            return (g * (1.0 / (1.0 + jnp.exp(-g))) * u).astype(BF16)

        act[slot, :, 0:256] = gate(product(wgu0, 0, 256), product(wgu0, 256, 256))
        act[slot, :, 256:512] = gate(product(wgu1, 0, 256), product(wgu1, 256, 256))
        both = product(wgu0, 512, 256)
        act[slot, :, 512:640] = gate(both[:, :128], both[:, 128:])
        both = product(wgu1, 512, 128)
        act[slot, :, 640:704] = gate(both, pltpu.roll(both, 64, 1))[:, :64]

    @pl.loop(0, 4)
    def feed(i):
        places = row_set(i)
        with jax.named_scope("feed_wait"):
            @pl.when(i == 0)
            def _():
                gather2.step1()
                complete(GU0)
                complete(GU1)

            @pl.when(i == 2)
            def _():
                third_phase(DOWN)
                gather2.step2()

        with jax.named_scope("feed_down"):
            @pl.when(i == 3)
            def _():
                gather2.step3()
                complete(DOWN)
                partial_out(act[1], wd, scatter2, row_set(1))
                partial_out(act[2], wd, scatter2, row_set(2))
                scatter2.near()

        with jax.named_scope("feed_from"):
            from_other(gather2, places)

        with jax.named_scope("gate_up"):
            gate_up(i, rows_of(n2, places))

    with jax.named_scope("rs2_far"):
        scatter2.far()
    with jax.named_scope("down_last"):
        partial_out(act[3], wd, scatter2, row_set(3))
    with jax.named_scope("down_own"):
        partial_out(act[0], wd, scatter2, row_set(0))
    with jax.named_scope("rs2_ready"):
        scatter2.ready()
    with jax.named_scope("rs2_through"):
        scatter2.through()
    with jax.named_scope("rs2_total"):
        for h in range(2):
            hidden[h] = hidden[h] + scatter2.own(h)
        for q in range(2):
            rows = pl.ds(q * 32, 32)
            values = hidden[:, rows] + scatter2.total(q)
            for h in range(2):
                out[pl.ds(h * 64 + q * 32, 32), :] = values[h]

    with jax.named_scope("drain"):
        for g in range(5):
            for phase in range(6):
                await_bytes(halves(g, phase), w_send.at[g, phase])
        gather1.drain()
        gather2.drain()
        scatter1.drain()
        scatter2.drain()


def per_device(
    tokens, mix_gain, w_query, w_key, w_value, w_decay_down, w_decay_up, decay_bias, decay_shift,
    head_gain, w_mix_out, ffn_gain, w_gate, w_up, w_down,
):
    hbm = pl.BlockSpec(memory_space=pltpu.HBM)
    vmem = pl.BlockSpec(memory_space=pltpu.VMEM)
    dma = pltpu.SemaphoreType.DMA
    scatter = [
        pltpu.VMEM((4, 2, 2, 64, 2048), BF16),
        pltpu.VMEM((4, 2, 64, 2048), BF16),
        pltpu.VMEM((2, 64, 2048), BF16),
        pltpu.VMEM((2, 2, 64, 2048), BF16),
    ]
    return pl.pallas_call(
        kernel,
        out_shape=pltpu.VMEM((128, 2048), F32),
        in_specs=[hbm] * 9 + [vmem] * 6,
        out_specs=vmem,
        scratch_shapes=[
            *[pltpu.VMEM((4, 4, 4, *quarter), BF16) for quarter in QUARTERS],
            pltpu.VMEM((704, 128), BF16),
            pltpu.VMEM((704, 128), BF16),
            pltpu.VMEM((128, 2048), BF16),
            pltpu.VMEM((16, BLK, 128), F32),
            pltpu.VMEM((16, BLK, 128), F32),
            pltpu.VMEM((4, 2, 2, 64, 2048), BF16),
            pltpu.VMEM((4, 2, 2, 64, 2048), BF16),
            pltpu.VMEM((16, BLK, 128), BF16),
            pltpu.VMEM((16, BLK, 128), BF16),
            pltpu.VMEM((16, BLK, DV), BF16),
            pltpu.VMEM((16, BLK, DV), BF16),
            pltpu.VMEM((256, 128), F32),
            pltpu.VMEM((2, 64, 2048), F32),
            pltpu.VMEM((4, 256, 704), BF16),
            *scatter, *scatter,
            dma((9,)), dma((5, 6)), dma((5, 6)),
            dma((20,)), dma((4, 2, 2)), dma((20,)), dma((4, 2, 2)),
            dma((4, 2)), dma((4, 2)), dma((10,)), dma((10,)),
            dma((4, 2)), dma((4, 2)), dma((10,)), dma((10,)),
        ],
        compiler_params=pltpu.CompilerParams(
            collective_id=0, has_side_effects=True, vmem_limit_bytes=58 * 1024 * 1024
        ),
    )(
        tokens,
        decay_shift.reshape(16, BLK, 128),
        w_query.reshape(4, 32, 128),
        w_key.reshape(4, 32, 128),
        w_value.reshape(4, 32, 256),
        w_mix_out.reshape(4, 64, 128),
        w_gate.T,
        w_up.T,
        w_down.reshape(4, 176, 128),
        mix_gain.reshape(1, -1),
        ffn_gain.reshape(1, -1),
        head_gain.reshape(1, -1),
        w_decay_down.T,
        w_decay_up,
        decay_bias.reshape(1, -1),
    )


def solution(mesh):
    finer = Mesh(mesh.devices.reshape(mesh.shape["rep"], 4, 4, 4, 2), AXES)
    everything, fs, tp = AXES, ("fz", "fx"), ("ty", "tc")
    return jax.shard_map(
        per_device,
        mesh=finer,
        in_specs=(
            P(everything, None), P(), P(fs, tp), P(fs, tp), P(fs, tp), P(), P(), P(),
            P(("rep", *fs), tp), P(), P(tp, fs), P(), P(fs, tp), P(fs, tp), P(tp, fs),
        ),
        out_specs=P(everything, None),
        check_vma=False,
    )
```

```python
import jax
import jax.numpy as jnp
from jax import lax
from jax.experimental import pallas as pl
from jax.experimental.pallas import tpu as pltpu
from jax.sharding import Mesh
from jax.sharding import PartitionSpec as P

AXES = ("rep", "fz", "fx", "ty", "tc")
MESH = pl.DeviceIdType.MESH
KEY_CHANNELS = 128
DV = 256
BLK = 64
EPS = 1e-06
TAU = 16.0
F32 = jnp.float32
BF16 = jnp.bfloat16
NT = (((1,), (1,)), ((), ()))
TN = (((0,), (0,)), ((), ()))
QKV, OUT, GU0, GU1, DOWN = range(5)
QUARTERS = ((32, 512), (64, 128), (32, 768), (32, 640), (176, 128))


def rms_norm(values, gain):
    return values * lax.rsqrt(jnp.mean(values * values, axis=-1, keepdims=True) + EPS) * gain


def dot(a, b, dims=(((1,), (0,)), ((), ()))):
    return lax.dot_general(a, b, dims, preferred_element_type=F32)


def kernel(
    tokens_hbm, shift_hbm, wq_hbm, wk_hbm, wv_hbm, wo_hbm, wg_hbm, wu_hbm, wd_hbm,
    mix_gain, ffn_gain, head_gain, down_proj, up_proj, bias,
    out,
    wqkv, wo, wgu0, wgu1, wd, gate_t, up_t,
    tok, shift, cums, n1, n2, qs, ks, vs, gated, state, hidden, act,
    part1, cross1, fold1, recv1, part2, cross2, fold2, recv2,
    loc_sem, w_send, w_recv,
    ag1_send, ag1_recv, ag2_send, ag2_recv,
    x1_send, x1_recv, r1_send, r1_recv, x2_send, x2_recv, r2_send, r2_recv,
):
    rep, fz, fx = lax.axis_index("rep"), lax.axis_index("fz"), lax.axis_index("fx")
    ty, tc = lax.axis_index("ty"), lax.axis_index("tc")
    tp = ty * 2 + tc
    weights = (wqkv, wo, wgu0, wgu1, wd)
    every = slice(None)

    def at_x(k):
        return {"fx": lax.rem(fx + k + 4, 4)}

    def at_z(k):
        whole = lax.rem(rep * 4 + fz + k + 8, 8)
        return {"rep": whole // 4, "fz": lax.rem(whole, 4)}

    def at_y(k):
        return {"ty": lax.rem(ty + k + 4, 4)}

    def chip_at(k):
        return lax.rem(ty + k + 4, 4)

    other = {"tc": 1 - tc}

    mine = [
        pltpu.make_async_copy(tokens_hbm, tok, loc_sem.at[0]),
        pltpu.make_async_copy(wq_hbm, wqkv.at[fz, fx, :, :, pl.ds(0, 128)], loc_sem.at[1]),
        pltpu.make_async_copy(wk_hbm, wqkv.at[fz, fx, :, :, pl.ds(128, 128)], loc_sem.at[2]),
        pltpu.make_async_copy(wv_hbm, wqkv.at[fz, fx, :, :, pl.ds(256, 256)], loc_sem.at[3]),
        pltpu.make_async_copy(wo_hbm, wo.at[fz, fx], loc_sem.at[4]),
        pltpu.make_async_copy(wg_hbm, gate_t, loc_sem.at[5]),
        pltpu.make_async_copy(wu_hbm, up_t, loc_sem.at[6]),
        pltpu.make_async_copy(wd_hbm, wd.at[fz, fx], loc_sem.at[7]),
        pltpu.make_async_copy(shift_hbm, shift, loc_sem.at[8]),
    ]
    for copy in mine:
        copy.start()

    barrier = pltpu.get_barrier_semaphore()
    peers = [at_x(1), at_x(2), at_x(3), at_z(1), at_z(-1), at_z(2), at_z(-2), at_y(1), at_y(3), other]
    for peer in peers:
        pl.semaphore_signal(barrier, inc=1, device_id=peer, device_id_type=MESH)

    mine[0].wait()
    normed = rms_norm(tok[...].astype(F32), mix_gain[...]).astype(BF16)
    n1[ty, tc] = normed.reshape(2, 64, 2048)
    for copy in mine[1:8]:
        copy.wait()

    pl.semaphore_wait(barrier, len(peers))

    def push(src, dst, send, recv, peer):
        pltpu.make_async_remote_copy(
            src_ref=src, dst_ref=dst, send_sem=send, recv_sem=recv, device_id=peer, device_id_type=MESH
        ).start()

    def await_bytes(view, sem):
        pltpu.make_async_copy(view, view, sem).wait()

    def spread(g, phase, z, x, first, count, peer):
        piece = weights[g].at[z, x, pl.ds(first, count)]
        push(piece, piece, w_send.at[g, phase], w_recv.at[g, phase], peer)

    def halves(g, phase):
        buf = weights[g]
        if phase < 2:
            return buf.at[0, pl.ds(0, 3), pl.ds(0, 2)]
        if phase < 4:
            return buf.at[pl.ds(0, 2), :, pl.ds(0, 2)]
        return buf.at[0, :, pl.ds(0, 2)]

    def landed(g, *phases):
        for phase in phases:
            await_bytes(halves(g, phase), w_recv.at[g, phase])

    def first_phase(g):
        for k in (1, -1, 2):
            spread(g, 0, fz, fx, 0, 2, at_x(k))
        for k in (1, -1):
            spread(g, 1, fz, fx, 2, 2, at_z(k))
        spread(g, 1, fz, fx, 2, 1, at_z(2))
        spread(g, 1, fz, fx, 3, 1, at_z(-2))

    def second_phase(g):
        landed(g, 0, 1)
        for k in (1, -1):
            spread(g, 2, fz, every, 0, 2, at_z(k))
            spread(g, 3, every, fx, 2, 2, at_x(k))

    def third_phase(g):
        landed(g, 2, 3)
        spread(g, 4, lax.rem(fz + 3, 4), every, 0, 1, at_z(1))
        spread(g, 4, lax.rem(fz + 1, 4), every, 1, 1, at_z(-1))
        spread(g, 5, every, lax.rem(fx + 3, 4), 2, 1, at_x(1))
        spread(g, 5, every, lax.rem(fx + 1, 4), 3, 1, at_x(-1))

    def complete(g):
        landed(g, 4, 5)

    class Gather:
        def __init__(self, buf, send, recv):
            self.buf, self.send, self.recv = buf, send, recv

        def some(self, j, chip, core, h, first, count, peer):
            piece = self.buf.at[chip, core, h, pl.ds(first, count)]
            push(piece, piece, self.send.at[j], self.recv.at[chip, core, h], peer)

        def half(self, j, chip, core, h, peer):
            self.some(j, chip, core, h, 0, 64, peer)

        def came(self, chip, core, h):
            await_bytes(self.buf.at[chip, core, h], self.recv.at[chip, core, h])

        def start(self, q):
            rows = pl.ds(q * 32, 32)
            own, ahead, back = self.buf.at[ty, tc], at_y(1), at_y(-1)
            plan = [(0, ahead), (1, back), (0, other), (1, other)]
            for j, (h, peer) in enumerate(plan):
                push(own.at[h, rows], own.at[h, rows], self.send.at[q * 4 + j], self.recv.at[ty, tc, h], peer)
            if q == 1:
                self.some(14, ty, tc, 1, 0, 32, ahead)
                self.some(15, ty, tc, 0, 0, 32, back)

        def step1(self):
            back, ahead = chip_at(-1), chip_at(1)
            self.came(back, tc, 0)
            self.half(8, back, tc, 0, at_y(1))
            self.some(16, ty, tc, 1, 32, 32, at_y(1))
            self.half(9, back, tc, 0, other)
            self.came(ahead, tc, 1)
            self.half(18, ahead, tc, 1, at_y(-1))
            self.some(17, ty, tc, 0, 32, 32, at_y(-1))
            self.half(19, ahead, tc, 1, other)

        def step2(self):
            far = chip_at(2)
            self.came(far, tc, 0)
            self.half(12, far, tc, 0, other)
            self.came(far, tc, 1)
            self.half(13, far, tc, 1, other)

        def step3(self):
            back, ahead = chip_at(-1), chip_at(1)
            self.came(back, tc, 1)
            self.half(10, back, tc, 1, other)
            self.came(ahead, tc, 0)
            self.half(11, ahead, tc, 0, other)

        def theirs(self, chip):
            self.came(chip, 1 - tc, 0)
            self.came(chip, 1 - tc, 1)

        def drain(self):
            for j in range(20):
                whole = j in (8, 9, 10, 11, 12, 13, 18, 19)
                await_bytes(self.buf.at[0, 0, 0, pl.ds(0, 64 if whole else 32)], self.send.at[j])

    class Scatter:
        def __init__(self, part, cross, fold, recv, x_send, x_recv, r_send, r_recv):
            self.part, self.cross, self.fold, self.recv = part, cross, fold, recv
            self.x_send, self.x_recv, self.r_send, self.r_recv = x_send, x_recv, r_send, r_recv

        def swap(self, chip, h):
            push(
                self.part.at[chip, 1 - tc, h], self.cross.at[chip, h],
                self.x_send.at[chip, h], self.x_recv.at[chip, h], other,
            )

        def both(self, chip, h):
            await_bytes(self.cross.at[chip, h], self.x_recv.at[chip, h])
            return self.part[chip, tc, h].astype(F32) + self.cross[chip, h].astype(F32)

        def send(self, j, src, dst, k):
            push(src, dst, self.r_send.at[j], self.r_recv.at[j], at_y(k))

        def far(self):
            chip = chip_at(2)
            for h in range(2):
                self.part[chip, tc, h] = self.both(chip, h).astype(BF16)
            for q in range(2):
                rows = pl.ds(q * 32, 32)
                for h, k in ((0, 1), (1, -1)):
                    self.send(q * 2 + h, self.part.at[chip, tc, h, rows], self.fold.at[h, rows], k)

        def near(self):
            for d, h, k in ((0, 1, 1), (1, 0, -1)):
                chip = chip_at(k)
                self.part[chip, tc, h] = self.both(chip, h).astype(BF16)
                self.send(4 + d, self.part.at[chip, tc, h], self.recv.at[d, h], k)

        def ready(self):
            for h, k in ((0, 1), (1, -1)):
                chip = chip_at(k)
                self.part[chip, tc, h] = self.both(chip, h).astype(BF16)

        def through(self):
            for q in range(2):
                rows = pl.ds(q * 32, 32)
                for d, k in ((0, 1), (1, -1)):
                    chip = chip_at(k)
                    await_bytes(self.fold.at[d, rows], self.r_recv.at[q * 2 + d])
                    whole = self.part[chip, tc, d, rows].astype(F32) + self.fold[d, rows].astype(F32)
                    self.part[chip, tc, d, rows] = whole.astype(BF16)
                    self.send(6 + q * 2 + d, self.part.at[chip, tc, d, rows], self.recv.at[d, d, rows], k)

        def total(self, q):
            rows = pl.ds(q * 32, 32)
            for d in range(2):
                if q == 0:
                    await_bytes(self.recv.at[d, 1 - d], self.r_recv.at[4 + d])
                await_bytes(self.recv.at[d, d, rows], self.r_recv.at[6 + q * 2 + d])
            return self.recv[0, :, rows].astype(F32) + self.recv[1, :, rows].astype(F32)

        def own(self, h):
            return self.both(ty, h)

        def drain(self):
            for chip in range(4):
                for h in range(2):
                    await_bytes(self.cross.at[chip, h], self.x_send.at[chip, h])
            for j in range(10):
                await_bytes(self.fold.at[0, pl.ds(0, 64 if j in (4, 5) else 32)], self.r_send.at[j])

    gather1 = Gather(n1, ag1_send, ag1_recv)
    gather2 = Gather(n2, ag2_send, ag2_recv)
    scatter1 = Scatter(part1, cross1, fold1, recv1, x1_send, x1_recv, r1_send, r1_recv)
    scatter2 = Scatter(part2, cross2, fold2, recv2, x2_send, x2_recv, r2_send, r2_recv)

    with jax.named_scope("start"):
        gather1.start(0)
        gather1.start(1)
        first_phase(QKV)
        first_phase(OUT)

    with jax.named_scope("turn"):
        def turned(ref, first):
            return ref[pl.ds(first, 256), :].T.reshape(4, 32, 256)

        def mixed(first, count):
            both = jnp.concatenate([gate_t[pl.ds(first, count), :], up_t[pl.ds(first, count), :]], axis=0)
            return both.T.reshape(4, 32, 2 * count)

        wgu0[fz, fx, :, :, 0:256] = turned(gate_t, 0)
        wgu0[fz, fx, :, :, 256:512] = turned(up_t, 0)
        wgu0[fz, fx, :, :, 512:768] = mixed(512, 128)
        wgu1[fz, fx, :, :, 0:256] = turned(gate_t, 256)
        wgu1[fz, fx, :, :, 256:512] = turned(up_t, 256)
        wgu1[fz, fx, :, :, 512:640] = mixed(640, 64)

    def row_set(i):
        chip_a = chip_at(jnp.where(i == 0, 0, jnp.where(i == 2, 2, -1)))
        chip_b = chip_at(jnp.where(i == 0, 0, jnp.where(i == 2, 2, 1)))
        h_a = jnp.where(i == 3, 1, 0)
        return [(chip_a, 0, h_a), (chip_a, 1, h_a), (chip_b, 0, 1 - h_a), (chip_b, 1, 1 - h_a)]

    def rows_of(buf, places):
        return jnp.concatenate([buf[place] for place in places], axis=0)

    def from_other(gather, places):
        for chip, _, h in places[::2]:
            gather.came(chip, 1 - tc, h)

    def block(place):
        chip, core, h = place
        return chip * 4 + core * 2 + h

    cols = pl.ds(pl.multiple_of(tp * 128, 128), 128)

    def causal_mask(size, dtype):
        ri = lax.broadcasted_iota(jnp.int32, (size, size), 0)
        ci = lax.broadcasted_iota(jnp.int32, (size, size), 1)
        return jnp.where((ri >= ci) & (ri // BLK == ci // BLK), 1.0, 0.0).astype(dtype)

    def decay(places):
        x = rows_of(n1, places)
        low = dot(x, down_proj[...], NT).astype(BF16)
        pre = dot(low, up_proj[:, cols]) + bias[:, cols]
        soft = jnp.minimum(pre, 0.0) - jnp.log1p(jnp.exp(-jnp.abs(pre)))
        logs = soft / TAU + jnp.concatenate([shift[block(place)] for place in places], axis=0)
        one = logs.astype(BF16)
        rest = logs - one.astype(F32)
        two = rest.astype(BF16)
        three = (rest - two.astype(F32)).astype(BF16)
        sums = dot(causal_mask(256, BF16), jnp.concatenate([one, two, three], axis=1))
        cum = sums[:, :128] + sums[:, 128:256] + sums[:, 256:]
        for p, place in enumerate(places):
            cums[block(place)] = cum[p * 64 : p * 64 + 64]

    with jax.named_scope("second_qkv"):
        second_phase(QKV)
    with jax.named_scope("decay0"):
        mine[8].wait()
        own_set, first_set = row_set(0), row_set(1)
        from_other(gather1, own_set)
        decay(own_set)
    with jax.named_scope("ag1_step1"):
        gather1.step1()
    with jax.named_scope("second_out"):
        second_phase(OUT)
    with jax.named_scope("third_qkv"):
        third_phase(QKV)
        first_phase(GU0)
    with jax.named_scope("decay1"):
        from_other(gather1, first_set)
        decay(first_set)
    with jax.named_scope("ag1_step2"):
        gather1.step2()
    with jax.named_scope("third_out"):
        third_phase(OUT)
        first_phase(GU1)
    with jax.named_scope("complete_qkv"):
        complete(QKV)

    @pl.loop(0, 4)
    def project(i):
        places = row_set(i)
        with jax.named_scope("project_wait"):
            @pl.when(i == 2)
            def _():
                gather1.step3()

        with jax.named_scope("decay"):
            @pl.when(i > 1)
            def _():
                from_other(gather1, places)
                decay(places)

        with jax.named_scope("project"):
            x = rows_of(n1, places)
            both = dot(x, wqkv[:, :, :, :, pl.ds(0, 256)].reshape(2048, 256)).astype(BF16)
            values = dot(x, wqkv[:, :, :, :, pl.ds(256, 256)].reshape(2048, 256)).astype(BF16)
            for p, place in enumerate(places):
                piece = slice(p * 64, p * 64 + 64)
                qs[block(place)] = both[piece, :128]
                ks[block(place)] = both[piece, 128:]
                vs[block(place)] = values[piece]

    with jax.named_scope("second_gu0"):
        second_phase(GU0)
        first_phase(DOWN)

    causal = causal_mask(128, F32)
    state[...] = jnp.zeros_like(state)
    gain_row = head_gain[:, pl.ds(pl.multiple_of(tp * DV, DV), DV)]

    def attend(i):
        pair = pl.ds(i * 2, 2)
        cum = cums[pair].reshape(128, 128)
        v = vs[pair].reshape(128, DV)
        k = ks[pair].reshape(128, 128).astype(F32)
        q_full = qs[pair].reshape(128, 128).astype(F32) * KEY_CHANNELS ** (-0.5) * jnp.exp(cum)
        k_full = k * jnp.exp(-cum)
        q_dec, k_dec = q_full.astype(BF16), k_full.astype(BF16)
        q_low = (q_full - q_dec.astype(F32)).astype(BF16)
        k_low = (k_full - k_dec.astype(F32)).astype(BF16)
        scores = dot(
            jnp.concatenate([q_dec, q_dec, q_low], axis=1),
            jnp.concatenate([k_dec, k_low, k_dec], axis=1), NT,
        )
        scores = jnp.where(causal > 0.5, scores, 0.0).astype(BF16)
        inner = dot(scores, v)
        s = state[...]
        carried = []
        for b in range(2):
            part = slice(b * BLK, (b + 1) * BLK)
            tot = cum[(b + 1) * BLK - 1 : (b + 1) * BLK, :]
            carried.append(dot(q_dec[part], s.astype(BF16), NT))
            weighted = (k[part] * jnp.exp(tot - cum[part])).astype(BF16)
            s = jnp.exp(tot) * s + dot(v[part], weighted, TN)
        state[...] = s
        head = inner + jnp.concatenate(carried, axis=0)
        gated[pair] = rms_norm(head, gain_row).astype(BF16).reshape(2, BLK, DV)

    with jax.named_scope("attend"):
        pl.loop(0, 8, unroll=2)(attend)
    with jax.named_scope("complete_out"):
        complete(OUT)

    def partial_out(x, buf, scatter, places):
        for f in range(0, 16, 2):
            left, right = buf[f // 4, f % 4], buf[f // 4, f % 4 + 1]
            depth = left.shape[0] * left.shape[1]
            w = jnp.concatenate([left.reshape(depth, 128), right.reshape(depth, 128)], axis=1)
            product = dot(x, w).astype(BF16)
            for p, (chip, core, h) in enumerate(places):
                scatter.part[chip, core, h, :, f * 128 : f * 128 + 256] = product[p * 64 : p * 64 + 64]
        for chip, core, h in places:
            if core == 0:
                scatter.swap(chip, h)

    @pl.loop(0, 4)
    def mix(i):
        with jax.named_scope("mix"):
            chip = chip_at(jnp.where(i == 0, 2, jnp.where(i == 1, 1, jnp.where(i == 2, 3, 0))))
            x = gated[pl.ds(chip * 4, 4)].reshape(256, DV)
            partial_out(x, wo, scatter1, [(chip, 0, 0), (chip, 0, 1), (chip, 1, 0), (chip, 1, 1)])

    with jax.named_scope("rs1_far"):
        scatter1.far()
    with jax.named_scope("rs1_near"):
        scatter1.near()
        scatter1.ready()
        for h in range(2):
            own = tok[pl.ds(h * 64, 64), :].astype(F32) + scatter1.own(h)
            hidden[h] = own
    with jax.named_scope("second_gu1"):
        second_phase(GU1)
    with jax.named_scope("rs1_through"):
        scatter1.through()
    with jax.named_scope("third_gu0"):
        third_phase(GU0)
    with jax.named_scope("third_gu1"):
        third_phase(GU1)
        second_phase(DOWN)
    for q in range(2):
        with jax.named_scope("rs1_total"):
            rows = pl.ds(q * 32, 32)
            values = hidden[:, rows] + scatter1.total(q)
            hidden[:, rows] = values
            n2[ty, tc, :, rows] = rms_norm(values, ffn_gain[...]).astype(BF16)
            gather2.start(q)

    def gate_up(slot, x):
        def product(buf, first, width):
            return dot(x, buf[:, :, :, :, pl.ds(first, width)].reshape(2048, width))

        def gate(g, u):
            return (g * (1.0 / (1.0 + jnp.exp(-g))) * u).astype(BF16)

        act[slot, :, 0:256] = gate(product(wgu0, 0, 256), product(wgu0, 256, 256))
        act[slot, :, 256:512] = gate(product(wgu1, 0, 256), product(wgu1, 256, 256))
        both = product(wgu0, 512, 256)
        act[slot, :, 512:640] = gate(both[:, :128], both[:, 128:])
        both = product(wgu1, 512, 128)
        act[slot, :, 640:704] = gate(both, pltpu.roll(both, 64, 1))[:, :64]

    @pl.loop(0, 4)
    def feed(i):
        places = row_set(i)
        with jax.named_scope("feed_wait"):
            @pl.when(i == 0)
            def _():
                gather2.step1()
                complete(GU0)
                complete(GU1)

            @pl.when(i == 2)
            def _():
                third_phase(DOWN)
                gather2.step2()

        with jax.named_scope("feed_down"):
            @pl.when(i == 3)
            def _():
                gather2.step3()
                complete(DOWN)
                partial_out(act[1], wd, scatter2, row_set(1))
                partial_out(act[2], wd, scatter2, row_set(2))
                scatter2.near()

        with jax.named_scope("feed_from"):
            from_other(gather2, places)

        with jax.named_scope("gate_up"):
            gate_up(i, rows_of(n2, places))

    with jax.named_scope("rs2_far"):
        scatter2.far()
    with jax.named_scope("down_last"):
        partial_out(act[3], wd, scatter2, row_set(3))
    with jax.named_scope("down_own"):
        partial_out(act[0], wd, scatter2, row_set(0))
    with jax.named_scope("rs2_ready"):
        scatter2.ready()
    with jax.named_scope("rs2_through"):
        scatter2.through()
    with jax.named_scope("rs2_total"):
        for h in range(2):
            hidden[h] = hidden[h] + scatter2.own(h)
        for q in range(2):
            rows = pl.ds(q * 32, 32)
            values = hidden[:, rows] + scatter2.total(q)
            for h in range(2):
                out[pl.ds(h * 64 + q * 32, 32), :] = values[h]

    with jax.named_scope("drain"):
        for g in range(5):
            for phase in range(6):
                await_bytes(halves(g, phase), w_send.at[g, phase])
        gather1.drain()
        gather2.drain()
        scatter1.drain()
        scatter2.drain()


def per_device(
    tokens, mix_gain, w_query, w_key, w_value, w_decay_down, w_decay_up, decay_bias, decay_shift,
    head_gain, w_mix_out, ffn_gain, w_gate, w_up, w_down,
):
    hbm = pl.BlockSpec(memory_space=pltpu.HBM)
    vmem = pl.BlockSpec(memory_space=pltpu.VMEM)
    dma = pltpu.SemaphoreType.DMA
    scatter = [
        pltpu.VMEM((4, 2, 2, 64, 2048), BF16),
        pltpu.VMEM((4, 2, 64, 2048), BF16),
        pltpu.VMEM((2, 64, 2048), BF16),
        pltpu.VMEM((2, 2, 64, 2048), BF16),
    ]
    return pl.pallas_call(
        kernel,
        out_shape=pltpu.VMEM((128, 2048), F32),
        in_specs=[hbm] * 9 + [vmem] * 6,
        out_specs=vmem,
        scratch_shapes=[
            *[pltpu.VMEM((4, 4, 4, *quarter), BF16) for quarter in QUARTERS],
            pltpu.VMEM((704, 128), BF16),
            pltpu.VMEM((704, 128), BF16),
            pltpu.VMEM((128, 2048), BF16),
            pltpu.VMEM((16, BLK, 128), F32),
            pltpu.VMEM((16, BLK, 128), F32),
            pltpu.VMEM((4, 2, 2, 64, 2048), BF16),
            pltpu.VMEM((4, 2, 2, 64, 2048), BF16),
            pltpu.VMEM((16, BLK, 128), BF16),
            pltpu.VMEM((16, BLK, 128), BF16),
            pltpu.VMEM((16, BLK, DV), BF16),
            pltpu.VMEM((16, BLK, DV), BF16),
            pltpu.VMEM((256, 128), F32),
            pltpu.VMEM((2, 64, 2048), F32),
            pltpu.VMEM((4, 256, 704), BF16),
            *scatter, *scatter,
            dma((9,)), dma((5, 6)), dma((5, 6)),
            dma((20,)), dma((4, 2, 2)), dma((20,)), dma((4, 2, 2)),
            dma((4, 2)), dma((4, 2)), dma((10,)), dma((10,)),
            dma((4, 2)), dma((4, 2)), dma((10,)), dma((10,)),
        ],
        compiler_params=pltpu.CompilerParams(
            collective_id=0, has_side_effects=True, vmem_limit_bytes=58 * 1024 * 1024
        ),
    )(
        tokens,
        decay_shift.reshape(16, BLK, 128),
        w_query.reshape(4, 32, 128),
        w_key.reshape(4, 32, 128),
        w_value.reshape(4, 32, 256),
        w_mix_out.reshape(4, 64, 128),
        w_gate.T,
        w_up.T,
        w_down.reshape(4, 176, 128),
        mix_gain.reshape(1, -1),
        ffn_gain.reshape(1, -1),
        head_gain.reshape(1, -1),
        w_decay_down.T,
        w_decay_up,
        decay_bias.reshape(1, -1),
    )


def solution(mesh):
    finer = Mesh(mesh.devices.reshape(mesh.shape["rep"], 4, 4, 4, 2), AXES)
    everything, fs, tp = AXES, ("fz", "fx"), ("ty", "tc")
    return jax.shard_map(
        per_device,
        mesh=finer,
        in_specs=(
            P(everything, None), P(), P(fs, tp), P(fs, tp), P(fs, tp), P(), P(), P(),
            P(("rep", *fs), tp), P(), P(tp, fs), P(), P(fs, tp), P(fs, tp), P(tp, fs),
        ),
        out_specs=P(everything, None),
        check_vma=False,
    )
```

```python
import jax
import jax.numpy as jnp
from jax import lax
from jax.experimental import pallas as pl
from jax.experimental.pallas import tpu as pltpu
from jax.sharding import Mesh
from jax.sharding import PartitionSpec as P

AXES = ("rep", "fz", "fx", "ty", "tc")
MESH = pl.DeviceIdType.MESH
KEY_CHANNELS = 128
DV = 256
BLK = 64
EPS = 1e-06
TAU = 16.0
F32 = jnp.float32
BF16 = jnp.bfloat16
NT = (((1,), (1,)), ((), ()))
TN = (((0,), (0,)), ((), ()))
QKV, OUT, GU0, GU1, DOWN = range(5)
QUARTERS = ((32, 512), (64, 128), (32, 768), (32, 640), (176, 128))


def rms_norm(values, gain):
    return values * lax.rsqrt(jnp.mean(values * values, axis=-1, keepdims=True) + EPS) * gain


def dot(a, b, dims=(((1,), (0,)), ((), ()))):
    return lax.dot_general(a, b, dims, preferred_element_type=F32)


def kernel(
    tokens_hbm, shift_hbm, wq_hbm, wk_hbm, wv_hbm, wo_hbm, wg_hbm, wu_hbm, wd_hbm,
    mix_gain, ffn_gain, head_gain, down_proj, up_proj, bias,
    out,
    wqkv, wo, wgu0, wgu1, wd, gate_t, up_t,
    tok, shift, cums, n1, n2, qs, ks, vs, gated, state, hidden, act,
    part1, cross1, fold1, recv1, part2, cross2, fold2, recv2,
    loc_sem, w_send, w_recv,
    ag1_send, ag1_recv, ag2_send, ag2_recv,
    x1_send, x1_recv, r1_send, r1_recv, x2_send, x2_recv, r2_send, r2_recv,
):
    rep, fz, fx = lax.axis_index("rep"), lax.axis_index("fz"), lax.axis_index("fx")
    ty, tc = lax.axis_index("ty"), lax.axis_index("tc")
    tp = ty * 2 + tc
    weights = (wqkv, wo, wgu0, wgu1, wd)
    every = slice(None)

    def at_x(k):
        return {"fx": lax.rem(fx + k + 4, 4)}

    def at_z(k):
        whole = lax.rem(rep * 4 + fz + k + 8, 8)
        return {"rep": whole // 4, "fz": lax.rem(whole, 4)}

    def at_y(k):
        return {"ty": lax.rem(ty + k + 4, 4)}

    def chip_at(k):
        return lax.rem(ty + k + 4, 4)

    other = {"tc": 1 - tc}

    mine = [
        pltpu.make_async_copy(tokens_hbm, tok, loc_sem.at[0]),
        pltpu.make_async_copy(wq_hbm, wqkv.at[fz, fx, :, :, pl.ds(0, 128)], loc_sem.at[1]),
        pltpu.make_async_copy(wk_hbm, wqkv.at[fz, fx, :, :, pl.ds(128, 128)], loc_sem.at[2]),
        pltpu.make_async_copy(wv_hbm, wqkv.at[fz, fx, :, :, pl.ds(256, 256)], loc_sem.at[3]),
        pltpu.make_async_copy(wo_hbm, wo.at[fz, fx], loc_sem.at[4]),
        pltpu.make_async_copy(wg_hbm, gate_t, loc_sem.at[5]),
        pltpu.make_async_copy(wu_hbm, up_t, loc_sem.at[6]),
        pltpu.make_async_copy(wd_hbm, wd.at[fz, fx], loc_sem.at[7]),
        pltpu.make_async_copy(shift_hbm, shift, loc_sem.at[8]),
    ]
    for copy in mine:
        copy.start()

    barrier = pltpu.get_barrier_semaphore()
    peers = [at_x(1), at_x(2), at_x(3), at_z(1), at_z(-1), at_z(2), at_z(-2), at_y(1), at_y(3), other]
    for peer in peers:
        pl.semaphore_signal(barrier, inc=1, device_id=peer, device_id_type=MESH)

    mine[0].wait()
    normed = rms_norm(tok[...].astype(F32), mix_gain[...]).astype(BF16)
    n1[ty, tc] = normed.reshape(2, 64, 2048)
    for copy in mine[1:8]:
        copy.wait()

    pl.semaphore_wait(barrier, len(peers))

    def push(src, dst, send, recv, peer):
        pltpu.make_async_remote_copy(
            src_ref=src, dst_ref=dst, send_sem=send, recv_sem=recv, device_id=peer, device_id_type=MESH
        ).start()

    def await_bytes(view, sem):
        pltpu.make_async_copy(view, view, sem).wait()

    def spread(g, phase, z, x, first, count, peer):
        piece = weights[g].at[z, x, pl.ds(first, count)]
        push(piece, piece, w_send.at[g, phase], w_recv.at[g, phase], peer)

    def halves(g, phase):
        buf = weights[g]
        if phase < 2:
            return buf.at[0, pl.ds(0, 3), pl.ds(0, 2)]
        if phase < 4:
            return buf.at[pl.ds(0, 2), :, pl.ds(0, 2)]
        return buf.at[0, :, pl.ds(0, 2)]

    def landed(g, *phases):
        for phase in phases:
            await_bytes(halves(g, phase), w_recv.at[g, phase])

    def first_phase(g):
        for k in (1, -1, 2):
            spread(g, 0, fz, fx, 0, 2, at_x(k))
        for k in (1, -1):
            spread(g, 1, fz, fx, 2, 2, at_z(k))
        spread(g, 1, fz, fx, 2, 1, at_z(2))
        spread(g, 1, fz, fx, 3, 1, at_z(-2))

    def second_phase(g):
        landed(g, 0, 1)
        for k in (1, -1):
            spread(g, 2, fz, every, 0, 2, at_z(k))
            spread(g, 3, every, fx, 2, 2, at_x(k))

    def third_phase(g):
        landed(g, 2, 3)
        spread(g, 4, lax.rem(fz + 3, 4), every, 0, 1, at_z(1))
        spread(g, 4, lax.rem(fz + 1, 4), every, 1, 1, at_z(-1))
        spread(g, 5, every, lax.rem(fx + 3, 4), 2, 1, at_x(1))
        spread(g, 5, every, lax.rem(fx + 1, 4), 3, 1, at_x(-1))

    def complete(g):
        landed(g, 4, 5)

    class Gather:
        def __init__(self, buf, send, recv):
            self.buf, self.send, self.recv = buf, send, recv

        def some(self, j, chip, core, h, first, count, peer):
            piece = self.buf.at[chip, core, h, pl.ds(first, count)]
            push(piece, piece, self.send.at[j], self.recv.at[chip, core, h], peer)

        def half(self, j, chip, core, h, peer):
            self.some(j, chip, core, h, 0, 64, peer)

        def came(self, chip, core, h):
            await_bytes(self.buf.at[chip, core, h], self.recv.at[chip, core, h])

        def start(self, q):
            rows = pl.ds(q * 32, 32)
            own, ahead, back = self.buf.at[ty, tc], at_y(1), at_y(-1)
            plan = [(0, ahead), (1, back), (0, other), (1, other)]
            for j, (h, peer) in enumerate(plan):
                push(own.at[h, rows], own.at[h, rows], self.send.at[q * 4 + j], self.recv.at[ty, tc, h], peer)
            if q == 1:
                self.some(14, ty, tc, 1, 0, 32, ahead)
                self.some(15, ty, tc, 0, 0, 32, back)

        def step1(self):
            back, ahead = chip_at(-1), chip_at(1)
            self.came(back, tc, 0)
            self.half(8, back, tc, 0, at_y(1))
            self.some(16, ty, tc, 1, 32, 32, at_y(1))
            self.half(9, back, tc, 0, other)
            self.came(ahead, tc, 1)
            self.half(18, ahead, tc, 1, at_y(-1))
            self.some(17, ty, tc, 0, 32, 32, at_y(-1))
            self.half(19, ahead, tc, 1, other)

        def step2(self):
            far = chip_at(2)
            self.came(far, tc, 0)
            self.half(12, far, tc, 0, other)
            self.came(far, tc, 1)
            self.half(13, far, tc, 1, other)

        def step3(self):
            back, ahead = chip_at(-1), chip_at(1)
            self.came(back, tc, 1)
            self.half(10, back, tc, 1, other)
            self.came(ahead, tc, 0)
            self.half(11, ahead, tc, 0, other)

        def theirs(self, chip):
            self.came(chip, 1 - tc, 0)
            self.came(chip, 1 - tc, 1)

        def drain(self):
            for j in range(20):
                whole = j in (8, 9, 10, 11, 12, 13, 18, 19)
                await_bytes(self.buf.at[0, 0, 0, pl.ds(0, 64 if whole else 32)], self.send.at[j])

    class Scatter:
        def __init__(self, part, cross, fold, recv, x_send, x_recv, r_send, r_recv):
            self.part, self.cross, self.fold, self.recv = part, cross, fold, recv
            self.x_send, self.x_recv, self.r_send, self.r_recv = x_send, x_recv, r_send, r_recv

        def swap(self, chip, h):
            push(
                self.part.at[chip, 1 - tc, h], self.cross.at[chip, h],
                self.x_send.at[chip, h], self.x_recv.at[chip, h], other,
            )

        def both(self, chip, h):
            await_bytes(self.cross.at[chip, h], self.x_recv.at[chip, h])
            return self.part[chip, tc, h].astype(F32) + self.cross[chip, h].astype(F32)

        def send(self, j, src, dst, k):
            push(src, dst, self.r_send.at[j], self.r_recv.at[j], at_y(k))

        def far(self):
            chip = chip_at(2)
            for h in range(2):
                self.part[chip, tc, h] = self.both(chip, h).astype(BF16)
            for q in range(2):
                rows = pl.ds(q * 32, 32)
                for h, k in ((0, 1), (1, -1)):
                    self.send(q * 2 + h, self.part.at[chip, tc, h, rows], self.fold.at[h, rows], k)

        def near(self):
            for d, h, k in ((0, 1, 1), (1, 0, -1)):
                chip = chip_at(k)
                self.part[chip, tc, h] = self.both(chip, h).astype(BF16)
                self.send(4 + d, self.part.at[chip, tc, h], self.recv.at[d, h], k)

        def ready(self):
            for h, k in ((0, 1), (1, -1)):
                chip = chip_at(k)
                self.part[chip, tc, h] = self.both(chip, h).astype(BF16)

        def through(self):
            for q in range(2):
                rows = pl.ds(q * 32, 32)
                for d, k in ((0, 1), (1, -1)):
                    chip = chip_at(k)
                    await_bytes(self.fold.at[d, rows], self.r_recv.at[q * 2 + d])
                    whole = self.part[chip, tc, d, rows].astype(F32) + self.fold[d, rows].astype(F32)
                    self.part[chip, tc, d, rows] = whole.astype(BF16)
                    self.send(6 + q * 2 + d, self.part.at[chip, tc, d, rows], self.recv.at[d, d, rows], k)

        def total(self, q):
            rows = pl.ds(q * 32, 32)
            for d in range(2):
                if q == 0:
                    await_bytes(self.recv.at[d, 1 - d], self.r_recv.at[4 + d])
                await_bytes(self.recv.at[d, d, rows], self.r_recv.at[6 + q * 2 + d])
            return self.recv[0, :, rows].astype(F32) + self.recv[1, :, rows].astype(F32)

        def own(self, h):
            return self.both(ty, h)

        def drain(self):
            for chip in range(4):
                for h in range(2):
                    await_bytes(self.cross.at[chip, h], self.x_send.at[chip, h])
            for j in range(10):
                await_bytes(self.fold.at[0, pl.ds(0, 64 if j in (4, 5) else 32)], self.r_send.at[j])

    gather1 = Gather(n1, ag1_send, ag1_recv)
    gather2 = Gather(n2, ag2_send, ag2_recv)
    scatter1 = Scatter(part1, cross1, fold1, recv1, x1_send, x1_recv, r1_send, r1_recv)
    scatter2 = Scatter(part2, cross2, fold2, recv2, x2_send, x2_recv, r2_send, r2_recv)

    with jax.named_scope("start"):
        gather1.start(0)
        gather1.start(1)
        first_phase(QKV)
        first_phase(OUT)

    with jax.named_scope("turn"):
        def turned(ref, first):
            return ref[pl.ds(first, 256), :].T.reshape(4, 32, 256)

        def mixed(first, count):
            both = jnp.concatenate([gate_t[pl.ds(first, count), :], up_t[pl.ds(first, count), :]], axis=0)
            return both.T.reshape(4, 32, 2 * count)

        wgu0[fz, fx, :, :, 0:256] = turned(gate_t, 0)
        wgu0[fz, fx, :, :, 256:512] = turned(up_t, 0)
        wgu0[fz, fx, :, :, 512:768] = mixed(512, 128)
        wgu1[fz, fx, :, :, 0:256] = turned(gate_t, 256)
        wgu1[fz, fx, :, :, 256:512] = turned(up_t, 256)
        wgu1[fz, fx, :, :, 512:640] = mixed(640, 64)

    def row_set(i):
        chip_a = chip_at(jnp.where(i == 0, 0, jnp.where(i == 2, 2, -1)))
        chip_b = chip_at(jnp.where(i == 0, 0, jnp.where(i == 2, 2, 1)))
        h_a = jnp.where(i == 3, 1, 0)
        return [(chip_a, 0, h_a), (chip_a, 1, h_a), (chip_b, 0, 1 - h_a), (chip_b, 1, 1 - h_a)]

    def rows_of(buf, places):
        return jnp.concatenate([buf[place] for place in places], axis=0)

    def from_other(gather, places):
        for chip, _, h in places[::2]:
            gather.came(chip, 1 - tc, h)

    def block(place):
        chip, core, h = place
        return chip * 4 + core * 2 + h

    cols = pl.ds(pl.multiple_of(tp * 128, 128), 128)

    def causal_mask(size, dtype):
        ri = lax.broadcasted_iota(jnp.int32, (size, size), 0)
        ci = lax.broadcasted_iota(jnp.int32, (size, size), 1)
        return jnp.where((ri >= ci) & (ri // BLK == ci // BLK), 1.0, 0.0).astype(dtype)

    def decay(places):
        x = rows_of(n1, places)
        low = dot(x, down_proj[...], NT).astype(BF16)
        pre = dot(low, up_proj[:, cols]) + bias[:, cols]
        soft = jnp.minimum(pre, 0.0) - jnp.log1p(jnp.exp(-jnp.abs(pre)))
        logs = soft / TAU + jnp.concatenate([shift[block(place)] for place in places], axis=0)
        one = logs.astype(BF16)
        rest = logs - one.astype(F32)
        two = rest.astype(BF16)
        three = (rest - two.astype(F32)).astype(BF16)
        sums = dot(causal_mask(256, BF16), jnp.concatenate([one, two, three], axis=1))
        cum = sums[:, :128] + sums[:, 128:256] + sums[:, 256:]
        for p, place in enumerate(places):
            cums[block(place)] = cum[p * 64 : p * 64 + 64]

    with jax.named_scope("second_qkv"):
        second_phase(QKV)
    with jax.named_scope("decay0"):
        mine[8].wait()
        own_set, first_set = row_set(0), row_set(1)
        from_other(gather1, own_set)
        decay(own_set)
    with jax.named_scope("ag1_step1"):
        gather1.step1()
    with jax.named_scope("second_out"):
        second_phase(OUT)
    with jax.named_scope("third_qkv"):
        third_phase(QKV)
        first_phase(GU0)
    with jax.named_scope("decay1"):
        from_other(gather1, first_set)
        decay(first_set)
    with jax.named_scope("ag1_step2"):
        gather1.step2()
    with jax.named_scope("third_out"):
        third_phase(OUT)
        first_phase(GU1)
    with jax.named_scope("complete_qkv"):
        complete(QKV)

    @pl.loop(0, 4)
    def project(i):
        places = row_set(i)
        with jax.named_scope("project_wait"):
            @pl.when(i == 2)
            def _():
                gather1.step3()

        with jax.named_scope("decay"):
            @pl.when(i > 1)
            def _():
                from_other(gather1, places)
                decay(places)

        with jax.named_scope("project"):
            x = rows_of(n1, places)
            both = dot(x, wqkv[:, :, :, :, pl.ds(0, 256)].reshape(2048, 256)).astype(BF16)
            values = dot(x, wqkv[:, :, :, :, pl.ds(256, 256)].reshape(2048, 256)).astype(BF16)
            for p, place in enumerate(places):
                piece = slice(p * 64, p * 64 + 64)
                qs[block(place)] = both[piece, :128]
                ks[block(place)] = both[piece, 128:]
                vs[block(place)] = values[piece]

    with jax.named_scope("second_gu0"):
        second_phase(GU0)
        first_phase(DOWN)

    causal = causal_mask(128, F32)
    state[...] = jnp.zeros_like(state)
    gain_row = head_gain[:, pl.ds(pl.multiple_of(tp * DV, DV), DV)]

    def attend(i):
        pair = pl.ds(i * 2, 2)
        cum = cums[pair].reshape(128, 128)
        v = vs[pair].reshape(128, DV)
        k = ks[pair].reshape(128, 128).astype(F32)
        q_full = qs[pair].reshape(128, 128).astype(F32) * KEY_CHANNELS ** (-0.5) * jnp.exp(cum)
        k_full = k * jnp.exp(-cum)
        q_dec, k_dec = q_full.astype(BF16), k_full.astype(BF16)
        q_low = (q_full - q_dec.astype(F32)).astype(BF16)
        k_low = (k_full - k_dec.astype(F32)).astype(BF16)
        scores = dot(
            jnp.concatenate([q_dec, q_dec, q_low], axis=1),
            jnp.concatenate([k_dec, k_low, k_dec], axis=1), NT,
        )
        scores = jnp.where(causal > 0.5, scores, 0.0).astype(BF16)
        inner = dot(scores, v)
        s = state[...]
        carried = []
        for b in range(2):
            part = slice(b * BLK, (b + 1) * BLK)
            tot = cum[(b + 1) * BLK - 1 : (b + 1) * BLK, :]
            carried.append(dot(q_dec[part], s.astype(BF16), NT))
            weighted = (k[part] * jnp.exp(tot - cum[part])).astype(BF16)
            s = jnp.exp(tot) * s + dot(v[part], weighted, TN)
        state[...] = s
        head = inner + jnp.concatenate(carried, axis=0)
        gated[pair] = rms_norm(head, gain_row).astype(BF16).reshape(2, BLK, DV)

    with jax.named_scope("attend"):
        pl.loop(0, 8, unroll=2)(attend)
    with jax.named_scope("complete_out"):
        complete(OUT)

    def partial_out(x, buf, scatter, places):
        for f in range(0, 16, 2):
            left, right = buf[f // 4, f % 4], buf[f // 4, f % 4 + 1]
            depth = left.shape[0] * left.shape[1]
            w = jnp.concatenate([left.reshape(depth, 128), right.reshape(depth, 128)], axis=1)
            product = dot(x, w).astype(BF16)
            for p, (chip, core, h) in enumerate(places):
                scatter.part[chip, core, h, :, f * 128 : f * 128 + 256] = product[p * 64 : p * 64 + 64]
        for chip, core, h in places:
            if core == 0:
                scatter.swap(chip, h)

    @pl.loop(0, 4)
    def mix(i):
        with jax.named_scope("mix"):
            chip = chip_at(jnp.where(i == 0, 2, jnp.where(i == 1, 1, jnp.where(i == 2, 3, 0))))
            x = gated[pl.ds(chip * 4, 4)].reshape(256, DV)
            partial_out(x, wo, scatter1, [(chip, 0, 0), (chip, 0, 1), (chip, 1, 0), (chip, 1, 1)])

    with jax.named_scope("rs1_far"):
        scatter1.far()
    with jax.named_scope("rs1_near"):
        scatter1.near()
        scatter1.ready()
        for h in range(2):
            own = tok[pl.ds(h * 64, 64), :].astype(F32) + scatter1.own(h)
            hidden[h] = own
    with jax.named_scope("second_gu1"):
        second_phase(GU1)
    with jax.named_scope("rs1_through"):
        scatter1.through()
    with jax.named_scope("third_gu0"):
        third_phase(GU0)
    with jax.named_scope("third_gu1"):
        third_phase(GU1)
        second_phase(DOWN)
    for q in range(2):
        with jax.named_scope("rs1_total"):
            rows = pl.ds(q * 32, 32)
            values = hidden[:, rows] + scatter1.total(q)
            hidden[:, rows] = values
            n2[ty, tc, :, rows] = rms_norm(values, ffn_gain[...]).astype(BF16)
            gather2.start(q)

    def gate_up(slot, x):
        def product(buf, first, width):
            return dot(x, buf[:, :, :, :, pl.ds(first, width)].reshape(2048, width))

        def gate(g, u):
            return (g * (1.0 / (1.0 + jnp.exp(-g))) * u).astype(BF16)

        act[slot, :, 0:256] = gate(product(wgu0, 0, 256), product(wgu0, 256, 256))
        act[slot, :, 256:512] = gate(product(wgu1, 0, 256), product(wgu1, 256, 256))
        both = product(wgu0, 512, 256)
        act[slot, :, 512:640] = gate(both[:, :128], both[:, 128:])
        both = product(wgu1, 512, 128)
        act[slot, :, 640:704] = gate(both, pltpu.roll(both, 64, 1))[:, :64]

    @pl.loop(0, 4)
    def feed(i):
        places = row_set(i)
        with jax.named_scope("feed_wait"):
            @pl.when(i == 0)
            def _():
                gather2.step1()
                complete(GU0)
                complete(GU1)

            @pl.when(i == 2)
            def _():
                third_phase(DOWN)
                gather2.step2()
                complete(DOWN)
                partial_out(act[1], wd, scatter2, row_set(1))

        with jax.named_scope("feed_down"):
            @pl.when(i == 3)
            def _():
                scatter2.near()
                gather2.step3()
                partial_out(act[2], wd, scatter2, row_set(2))

        with jax.named_scope("feed_from"):
            from_other(gather2, places)

        with jax.named_scope("gate_up"):
            gate_up(i, rows_of(n2, places))

    with jax.named_scope("rs2_far"):
        scatter2.far()
    with jax.named_scope("down_last"):
        partial_out(act[3], wd, scatter2, row_set(3))
    with jax.named_scope("down_own"):
        partial_out(act[0], wd, scatter2, row_set(0))
    with jax.named_scope("rs2_ready"):
        scatter2.ready()
    with jax.named_scope("rs2_through"):
        scatter2.through()
    with jax.named_scope("rs2_total"):
        for h in range(2):
            hidden[h] = hidden[h] + scatter2.own(h)
        for q in range(2):
            rows = pl.ds(q * 32, 32)
            values = hidden[:, rows] + scatter2.total(q)
            for h in range(2):
                out[pl.ds(h * 64 + q * 32, 32), :] = values[h]

    with jax.named_scope("drain"):
        for g in range(5):
            for phase in range(6):
                await_bytes(halves(g, phase), w_send.at[g, phase])
        gather1.drain()
        gather2.drain()
        scatter1.drain()
        scatter2.drain()


def per_device(
    tokens, mix_gain, w_query, w_key, w_value, w_decay_down, w_decay_up, decay_bias, decay_shift,
    head_gain, w_mix_out, ffn_gain, w_gate, w_up, w_down,
):
    hbm = pl.BlockSpec(memory_space=pltpu.HBM)
    vmem = pl.BlockSpec(memory_space=pltpu.VMEM)
    dma = pltpu.SemaphoreType.DMA
    scatter = [
        pltpu.VMEM((4, 2, 2, 64, 2048), BF16),
        pltpu.VMEM((4, 2, 64, 2048), BF16),
        pltpu.VMEM((2, 64, 2048), BF16),
        pltpu.VMEM((2, 2, 64, 2048), BF16),
    ]
    return pl.pallas_call(
        kernel,
        out_shape=pltpu.VMEM((128, 2048), F32),
        in_specs=[hbm] * 9 + [vmem] * 6,
        out_specs=vmem,
        scratch_shapes=[
            *[pltpu.VMEM((4, 4, 4, *quarter), BF16) for quarter in QUARTERS],
            pltpu.VMEM((704, 128), BF16),
            pltpu.VMEM((704, 128), BF16),
            pltpu.VMEM((128, 2048), BF16),
            pltpu.VMEM((16, BLK, 128), F32),
            pltpu.VMEM((16, BLK, 128), F32),
            pltpu.VMEM((4, 2, 2, 64, 2048), BF16),
            pltpu.VMEM((4, 2, 2, 64, 2048), BF16),
            pltpu.VMEM((16, BLK, 128), BF16),
            pltpu.VMEM((16, BLK, 128), BF16),
            pltpu.VMEM((16, BLK, DV), BF16),
            pltpu.VMEM((16, BLK, DV), BF16),
            pltpu.VMEM((256, 128), F32),
            pltpu.VMEM((2, 64, 2048), F32),
            pltpu.VMEM((4, 256, 704), BF16),
            *scatter, *scatter,
            dma((9,)), dma((5, 6)), dma((5, 6)),
            dma((20,)), dma((4, 2, 2)), dma((20,)), dma((4, 2, 2)),
            dma((4, 2)), dma((4, 2)), dma((10,)), dma((10,)),
            dma((4, 2)), dma((4, 2)), dma((10,)), dma((10,)),
        ],
        compiler_params=pltpu.CompilerParams(
            collective_id=0, has_side_effects=True, vmem_limit_bytes=58 * 1024 * 1024
        ),
    )(
        tokens,
        decay_shift.reshape(16, BLK, 128),
        w_query.reshape(4, 32, 128),
        w_key.reshape(4, 32, 128),
        w_value.reshape(4, 32, 256),
        w_mix_out.reshape(4, 64, 128),
        w_gate.T,
        w_up.T,
        w_down.reshape(4, 176, 128),
        mix_gain.reshape(1, -1),
        ffn_gain.reshape(1, -1),
        head_gain.reshape(1, -1),
        w_decay_down.T,
        w_decay_up,
        decay_bias.reshape(1, -1),
    )


def solution(mesh):
    finer = Mesh(mesh.devices.reshape(mesh.shape["rep"], 4, 4, 4, 2), AXES)
    everything, fs, tp = AXES, ("fz", "fx"), ("ty", "tc")
    return jax.shard_map(
        per_device,
        mesh=finer,
        in_specs=(
            P(everything, None), P(), P(fs, tp), P(fs, tp), P(fs, tp), P(), P(), P(),
            P(("rep", *fs), tp), P(), P(tp, fs), P(), P(fs, tp), P(fs, tp), P(tp, fs),
        ),
        out_specs=P(everything, None),
        check_vma=False,
    )
```
